128 devices in a mesh: sp: 64 (over z, y, x), tp: 2 (over core).
Axes of the slice: x: 4, y: 4, z: 4, core: 2. Of those that a mesh axis runs over, the one named last changes fastest.
Arguments:
- features: bfloat16 [32768, 4096], P('sp', 'tp'), may hold values from -16 to 16
- weight_value: bfloat16 [4096, 1024], P(None, 'tp'), may hold values from -0.09375 to 0.09375
- weight_gate: bfloat16 [4096, 1024], P(None, 'tp'), may hold values from -0.09375 to 0.09375
- weight_out: bfloat16 [4096, 1024], P(None, 'tp'), may hold values from -0.1875 to 0.1875
- conv_taps: float32 [31, 1024], P(None, 'tp'), may hold values from -6 to 6
- norm_gain: float32 [1024], P('tp'), may hold values from 0.1 to 1.9
- out_grad: bfloat16 [32768, 4096], P('sp', 'tp'), may hold values from -16 to 16
Outputs:
- value_grad: float32 [32768, 1024], P('sp', 'tp')
- gate_grad: float32 [32768, 1024], P('sp', 'tp')
- value_wgrad: float32 [4096, 1024], P('sp', 'tp')
- gate_wgrad: float32 [4096, 1024], P('sp', 'tp')
- out_wgrad: float32 [4096, 1024], P('sp', 'tp')
- taps_grad: float32 [31, 1024], P(None, 'tp')
- gain_grad: float32 [1024], P('tp')
The draws below stay inside these ranges and needn't reach their ends.
All inputs are finite; a program needn't handle non-finite values.
Results may differ from the reference program's by a relative error of at most 0.0057.
Values may be sent and summed in bfloat16 or wider, within the bound.
A program may use at most 192 MiB of HBM per device.

```python
import math
import jax
import jax.numpy as jnp
from jax import lax

D = 4096
CH = 1024
KW = 31
TOKENS = 32768


def draw_conv_taps(key, part):
    base_key = jax.random.fold_in(key, 11)
    first_key, second_key, third_key = jax.random.split(base_key, 3)
    base = jnp.clip(jax.random.normal(first_key, (KW, CH), jnp.float32), -3.5, 3.5)
    spread = jnp.exp(jax.random.uniform(second_key, (CH,), jnp.float32, -0.7, 0.7))
    upper_big = jax.random.bernoulli(third_key)
    lower_half = jnp.arange(CH) < CH // 2
    block_scale = jnp.where(lower_half == upper_big, 3.5, 1.0)
    return base * spread * block_scale / math.sqrt(KW)


def strengthened(entries, own_key, source, target, shards_of, factor):
    owner, partner = [(jnp.arange(entries.shape[position]) // (entries.shape[position] // shards_of)).reshape([-1 if axis == position else 1 for axis in range(entries.ndim)]) for position in (source, target)]
    chosen = jax.random.permutation(own_key, shards_of)[partner]
    strong = (owner == chosen) | (owner == (partner + shards_of // 2) % shards_of)
    return jnp.where(strong, factor * entries, entries)


def shard_levels(key, shape, cuts, low, high):
    loudness = 1.0
    for position, blocks in cuts:
        heights = jax.random.uniform(jax.random.fold_in(jax.random.fold_in(key, 6), position), (blocks,), jnp.float32, low / len(cuts), high / len(cuts))
        loudness = loudness * jnp.repeat(jnp.exp(heights), shape[position] // blocks).reshape((-1,) + (1,) * (len(shape) - 1 - position))
    return loudness


def bell_draw(own_key, shape, deviation, most, cuts=(), held_as=jnp.bfloat16):
    result = deviation * jax.random.normal(own_key, shape, jnp.float32)
    if cuts:
        result = result * shard_levels(own_key, shape, cuts, -0.22, 0.18)
    return jnp.clip(result, -most, most).astype(held_as)


def noise_with(key, shape, scale, bound, shards, heavy, dtype=jnp.bfloat16):
    array = scale * jax.random.normal(key, shape, jnp.float32)
    if shards:
        array = array * shard_levels(key, shape, shards, -0.22, 0.18)
    return jnp.clip(strengthened(array, jax.random.fold_in(key, 3), *heavy), -bound, bound).astype(dtype)


def setup_inputs(seed: int = 0) -> dict:
    keys = jax.random.split(jax.random.key(seed), 8)
    return {
        "features": noise_with(keys[0], (TOKENS, D), 1.0, 16.0, ((0, 64), (1, 2)), (0, 1, 64, 4.0)),
        "weight_value": bell_draw(keys[1], (D, CH), D ** -0.5, 0.09375, ((1, 2),)),
        "weight_gate": bell_draw(keys[2], (D, CH), D ** -0.5, 0.09375, ((1, 2),)),
        "weight_out": bell_draw(keys[3], (D, CH), CH ** -0.5, 0.1875, ((1, 2),)),
        "conv_taps": draw_conv_taps(jax.random.fold_in(keys[7], 71), 0),
        "norm_gain": jnp.clip(1.0 + 0.18 * jax.random.normal(keys[5], (CH,), jnp.float32), 0.1, 1.9),
        "out_grad": noise_with(keys[6], (TOKENS, D), 1.0, 16.0, ((0, 64), (1, 2)), (0, 1, 64, 4.0)),
    }


NORM_EPS = 1e-05

def over_tokens(left_rows, right_rows):
    return lax.dot_general(left_rows, right_rows, (((0,), (0,)), ((), ())), preferred_element_type=jnp.float32)

def reference(features, weight_value, weight_gate, weight_out, conv_taps, norm_gain, out_grad):
    half_width = KW // 2
    seq_total = features.shape[0]
    value_half = jnp.dot(features, weight_value, preferred_element_type=jnp.float32).astype(jnp.bfloat16)
    gate_half = jnp.dot(features, weight_gate, preferred_element_type=jnp.float32).astype(jnp.bfloat16)
    value_half, gate_half = lax.optimization_barrier((value_half, gate_half))
    value_pre = value_half.astype(jnp.float32)
    gate_pre = gate_half.astype(jnp.float32)
    gate_sig = jax.nn.sigmoid(gate_pre)
    mixed_half = lax.optimization_barrier((value_pre * gate_sig).astype(jnp.bfloat16))
    padded = jnp.pad(mixed_half.astype(jnp.float32), ((half_width, half_width), (0, 0)))
    conv_out = jnp.zeros((seq_total, CH), jnp.float32)
    for offset in range(KW):
        conv_out = conv_out + conv_taps[offset] * padded[offset:offset + seq_total]
    mean_row = lax.optimization_barrier(jnp.sum(conv_out, axis=-1, keepdims=True)) / CH
    var_row = lax.optimization_barrier(jnp.sum(conv_out * conv_out, axis=-1, keepdims=True)) / CH - mean_row * mean_row
    inv_std = lax.rsqrt(var_row + NORM_EPS)
    normed = (conv_out - mean_row) * inv_std
    pre_act = normed * norm_gain
    act_sig = jax.nn.sigmoid(pre_act)
    act_half = (pre_act * act_sig).astype(jnp.bfloat16)
    act_grad = jnp.dot(out_grad, weight_out, preferred_element_type=jnp.float32)
    out_wgrad = over_tokens(out_grad, act_half)
    pre_grad = act_grad * act_sig * (1.0 + pre_act * (1.0 - act_sig))
    gain_grad = lax.optimization_barrier(jnp.sum(pre_grad * normed, axis=0))
    norm_grad = pre_grad * norm_gain
    first_mom = lax.optimization_barrier(jnp.sum(norm_grad, axis=-1, keepdims=True)) / CH
    second_mom = lax.optimization_barrier(jnp.sum(norm_grad * normed, axis=-1, keepdims=True)) / CH
    conv_grad = inv_std * (norm_grad - first_mom - normed * second_mom)
    grad_ext = jnp.pad(conv_grad, ((half_width, half_width), (0, 0)))
    mixed_grad = jnp.zeros((seq_total, CH), jnp.float32)
    taps_rows = []
    for offset in range(KW):
        begin = 2 * half_width - offset
        mixed_grad = mixed_grad + conv_taps[offset] * grad_ext[begin:begin + seq_total]
        taps_rows.append(lax.optimization_barrier(jnp.sum(conv_grad * padded[offset:offset + seq_total], axis=0)))
    taps_grad = jnp.stack(taps_rows)
    value_grad = mixed_grad * gate_sig
    gate_grad = mixed_grad * value_pre * gate_sig * (1.0 - gate_sig)
    value_wgrad = over_tokens(features, value_grad.astype(jnp.bfloat16))
    gate_wgrad = over_tokens(features, gate_grad.astype(jnp.bfloat16))
    return (value_grad, gate_grad, value_wgrad, gate_wgrad, out_wgrad, taps_grad, gain_grad)
```

```python
import jax
import jax.numpy as jnp
from jax import lax
from jax.sharding import Mesh
from jax.sharding import PartitionSpec as P

SP = ("sp_0", "sp_1", "sp_2")


NORM_EPS = 1e-05


def sum_by_axis(running, axes):
    for axis in axes:
        running = lax.psum_scatter(running, axis, scatter_dimension=0, tiled=True)
    return running


def in_one_piece(arrays, axis, dim, along):
    ends, at = ([], 0)
    for a in arrays[:-1]:
        at += a.shape[along]
        ends.append(at)
    both = jnp.concatenate(arrays, axis=along)
    return tuple(jnp.split(lax.all_gather(both, axis, axis=dim, tiled=True), ends, axis=along))


def with_halo(block, sides, width):
    for axis, dim in sides:
        count = lax.axis_size(axis)
        forward = [(i, i + 1) for i in range(count - 1)]
        backward = [(target, source) for source, target in forward]
        low = lax.ppermute(
            lax.slice_in_dim(block, block.shape[dim] - width, None, axis=dim), axis, forward
        )
        high = lax.ppermute(lax.slice_in_dim(block, 0, width, axis=dim), axis, backward)
        block = jnp.concatenate([low, block, high], axis=dim)
    return block


def from_everyone(x, axis):
    devices = lax.axis_size(axis)
    return lax.all_to_all(jnp.broadcast_to(x[None], (devices, *x.shape)), axis, 0, 0, tiled=True)


def of_everyone(x, axis):
    return from_everyone(x, axis).sum(axis=0)


def packed_total(arrays, axis):
    vector, at, finished = (jnp.concatenate([a.reshape(-1) for a in arrays]), 0, [])
    running = of_everyone(vector, axis)
    for a in arrays:
        finished.append(running[at : at + a.size].reshape(a.shape))
        at += a.size
    return tuple(finished)


def total_of_pieces(x, axis):
    return lax.all_gather(x, axis).sum(0)


def make_term(left_rows, right_rows):
    return lax.dot_general(
        left_rows, right_rows, (((0,), (0,)), ((), ())), preferred_element_type=jnp.float32
    )


def out_weight_sum(whole_cotangent, act_half):
    term = make_term(whole_cotangent, act_half).astype(jnp.bfloat16)
    return sum_by_axis(term, SP).astype(jnp.float32)


def on_device(features, weight_value, weight_gate, weight_out, conv_taps, norm_gain, out_grad):
    whole_inputs, whole_cotangent = in_one_piece((features, out_grad), "tp", 1, 0)
    value_half = jnp.dot(whole_inputs, weight_value, preferred_element_type=jnp.float32).astype(
        jnp.bfloat16
    )
    gate_half = jnp.dot(whole_inputs, weight_gate, preferred_element_type=jnp.float32).astype(
        jnp.bfloat16
    )
    value_half, gate_half = lax.optimization_barrier((value_half, gate_half))
    value_pre = value_half.astype(jnp.float32)
    gate_pre = gate_half.astype(jnp.float32)
    gate_sig = jax.nn.sigmoid(gate_pre)
    mixed_half = lax.optimization_barrier((value_pre * gate_sig).astype(jnp.bfloat16))
    tap_count = conv_taps.shape[0]
    half_width = tap_count // 2
    row_count = mixed_half.shape[0]
    channels = mixed_half.shape[1] * lax.axis_size("tp")
    extended = with_halo(mixed_half, ((SP, 0),), half_width).astype(jnp.float32)
    conv_out = jnp.zeros(mixed_half.shape, jnp.float32)
    for offset in range(tap_count):
        conv_out = conv_out + conv_taps[offset] * extended[offset : offset + row_count]
    row_sum, row_square = packed_total(
        (jnp.sum(conv_out, axis=-1), jnp.sum(conv_out * conv_out, axis=-1)), "tp"
    )
    mean_row = row_sum[:, None] / channels
    var_row = row_square[:, None] / channels - mean_row * mean_row
    inv_std = lax.rsqrt(var_row + NORM_EPS)
    normed = (conv_out - mean_row) * inv_std
    pre_act = normed * norm_gain
    act_sig = jax.nn.sigmoid(pre_act)
    act_half = (pre_act * act_sig).astype(jnp.bfloat16)
    act_grad = jnp.dot(whole_cotangent, weight_out, preferred_element_type=jnp.float32)
    pre_grad = act_grad * act_sig * (1.0 + pre_act * (1.0 - act_sig))
    gain_part = jnp.sum(pre_grad * normed, axis=0)
    norm_grad = pre_grad * norm_gain
    first_sum, second_sum = packed_total(
        (jnp.sum(norm_grad, axis=-1), jnp.sum(norm_grad * normed, axis=-1)), "tp"
    )
    first_mom = first_sum[:, None] / channels
    second_mom = second_sum[:, None] / channels
    conv_grad = inv_std * (norm_grad - first_mom - normed * second_mom)
    grad_ext = with_halo(conv_grad, ((SP, 0),), half_width)
    mixed_grad = jnp.zeros(conv_grad.shape, jnp.float32)
    taps_rows = []
    for offset in range(tap_count):
        begin = 2 * half_width - offset
        mixed_grad = mixed_grad + conv_taps[offset] * grad_ext[begin : begin + row_count]
        taps_rows.append(jnp.sum(conv_grad * extended[offset : offset + row_count], axis=0))
    small = lax.psum(jnp.concatenate([jnp.stack(taps_rows), gain_part[None]], axis=0), SP)
    taps_grad, gain_grad = small[:tap_count], small[tap_count]
    value_grad = mixed_grad * gate_sig
    gate_grad = mixed_grad * value_pre * gate_sig * (1.0 - gate_sig)
    value_low = value_grad.astype(jnp.bfloat16)
    gate_low = gate_grad.astype(jnp.bfloat16)
    out_wgrad = out_weight_sum(whole_cotangent, act_half)
    both_low = jnp.concatenate([value_low, gate_low], axis=1)
    joined = sum_by_axis(make_term(whole_inputs, both_low).astype(jnp.bfloat16), SP)
    joined = joined.astype(jnp.float32)
    split_at = value_low.shape[1]
    value_wgrad = joined[:, :split_at]
    gate_wgrad = joined[:, split_at:]
    return (value_grad, gate_grad, value_wgrad, gate_wgrad, out_wgrad, taps_grad, gain_grad)


def solution(mesh):
    split = Mesh(mesh.devices.reshape(4, 4, 4, mesh.shape["tp"]), ("sp_0", "sp_1", "sp_2", "tp"))
    return jax.shard_map(
        on_device,
        mesh=split,
        in_specs=(
            P(SP, "tp"),
            P(None, "tp"),
            P(None, "tp"),
            P(None, "tp"),
            P(None, "tp"),
            P("tp"),
            P(SP, "tp"),
        ),
        out_specs=(
            P(SP, "tp"),
            P(SP, "tp"),
            P(SP, "tp"),
            P(SP, "tp"),
            P(SP, "tp"),
            P(None, "tp"),
            P("tp"),
        ),
        check_vma=False,
    )
```

```python
import functools

import jax
import jax.numpy as jnp
from jax import lax
from jax.experimental import pallas as pl
from jax.experimental.pallas import tpu as pltpu
from jax.sharding import PartitionSpec as P

SP = "sp"
MESH = pl.DeviceIdType.MESH
BF16 = jnp.bfloat16
F32 = jnp.float32

NORM_EPS = 1e-05

WIDTHS = ((128, 128, 256), (256, 128, 128), (128, 256, 128))
ORDERS = ("xzy", "yxz", "zyx")
ROWS = (512, 128, 32)
SENT = (BF16, BF16, F32)


def coords():
    sp = lax.axis_index("sp")
    return {"z": sp // 16, "y": (sp // 4) % 4, "x": sp % 4}


def peer(where, dim, shift):
    to = dict(where)
    to[dim] = (where[dim] + shift + 4) % 4
    return (to["z"] * 16 + to["y"] * 4 + to["x"], lax.axis_index("tp"))


def remote(src, dst, ssem, rsem, device):
    return pltpu.make_async_remote_copy(
        src_ref=src, dst_ref=dst, send_sem=ssem, recv_sem=rsem,
        device_id=device, device_id_type=MESH,
    )


class Part:
    def __init__(self, where, p, lhs_t, rhs, cols, out, bufs, sems):
        self.where, self.p, self.lhs_t, self.rhs = where, p, lhs_t, rhs
        self.cols, self.out, self.bufs, self.sems = cols, out, bufs, sems

    def source(self, stage, h, j):
        off, width = self.cols
        if stage == 0:
            if self.p == 0:
                rows = self.lhs_t[pl.ds(2 * h, 2), :, j]
            elif self.p == 1:
                rows = self.lhs_t[:, j, pl.ds(2 * h, 2)]
            else:
                rows = self.lhs_t[j, pl.ds(2 * h, 2)]
            rows = rows.reshape(512, rows.shape[-1])
            return jnp.dot(rows, self.rhs[:, off : off + width], preferred_element_type=F32)
        held = self.bufs[stage - 1][2]
        if stage == 1:
            if self.p == 1:
                at = (j // 2) * 8 + j % 2
                two = [held[at + 2 * (2 * h + i)] for i in range(2)]
                return jnp.concatenate(two, axis=0)
            return held[pl.ds(4 * j + 2 * h, 2)].reshape(128, width)
        return held[j, pl.ds(pl.multiple_of(h * 32, 32), 32)]

    def place(self, stage, h, value):
        off, width = self.cols
        if stage == 2:
            self.out[pl.ds(pl.multiple_of(h * 32, 32), 32), off : off + width] = value
            return
        held = self.bufs[stage][2]
        count = ROWS[stage] // 64
        held[pl.ds(count * h, count)] = value.reshape(count, 64, width)

    def copy(self, stage, slot, sign):
        send, recv, _ = self.bufs[stage]
        ssem, rsem = self.sems
        at = stage * 6 + slot
        dim = ORDERS[self.p][stage]
        return remote(
            send.at[slot], recv.at[slot], ssem.at[at], rsem.at[at],
            peer(self.where, dim, sign),
        )

    def first(self, stage):
        m = self.where[ORDERS[self.p][stage]]
        send = self.bufs[stage][0]

        @pl.loop(0, 4)
        def _(i):
            sign = 1 - 2 * (i % 2)
            h = ((i + 1) // 2) % 2
            j = (m + 6 - (i // 2) * sign) % 4
            send[i] = self.source(stage, h, j).astype(SENT[stage])
            self.copy(stage, i, sign).start()

    def second(self, stage):
        m = self.where[ORDERS[self.p][stage]]
        send, recv, _ = self.bufs[stage]

        @pl.loop(0, 2)
        def _(k):
            sign = 1 - 2 * k
            self.copy(stage, k, sign).wait_recv()
            mine = self.source(stage, k, (m + 4 + sign) % 4)
            send[4 + k] = (mine + recv[k].astype(F32)).astype(SENT[stage])
            self.copy(stage, 4 + k, sign).start()

    def third(self, stage):
        m = self.where[ORDERS[self.p][stage]]
        recv = self.bufs[stage][1]

        @pl.loop(0, 2)
        def _(h):
            mine = self.source(stage, h, m)
            self.copy(stage, 3 - h, 1).wait_recv()
            self.copy(stage, 4 + h, 1).wait_recv()
            total = mine + recv[3 - h].astype(F32) + recv[4 + h].astype(F32)
            self.place(stage, h, total)

    def drain(self):
        for stage in range(3):
            @pl.loop(0, 6)
            def _(slot):
                self.copy(stage, slot, 1).wait_send()


class Small:
    def __init__(self, where, start, cols, slots, sums, out, sems):
        self.where, self.start, self.cols, self.slots = where, start, cols, slots
        self.sums, self.out, self.sems = sums, out, sems

    def copy(self, stage, d):
        dim = "xyzx"[stage]
        mine = self.where[dim]
        ssem, rsem = self.sems
        src = self.cols.at[(mine + d) % 4] if stage == 0 else self.sums.at[stage - 1]
        at = stage * 4 + d
        return remote(src, self.slots.at[stage, mine], ssem.at[at], rsem.at[at],
                      peer(self.where, dim, d))

    def send(self, stage):
        mine = self.where["xyzx"[stage]]
        if stage == 0:
            for j in range(4):
                self.cols[j] = self.start[:, 128 * j : 128 * j + 128]
            self.slots[0, mine] = self.cols[mine]
        else:
            self.slots[stage, mine] = self.sums[stage - 1]

        @pl.loop(1, 4)
        def _(d):
            self.copy(stage, d).start()

    def collect(self, stage):
        @pl.loop(1, 4)
        def _(d):
            self.copy(stage, d).wait_recv()

        if stage < 3:
            a, b, c, d = [self.slots[stage, j] for j in range(4)]
            self.sums[stage] = (a + b) + (c + d)
        else:
            for j in range(4):
                self.out[:, 128 * j : 128 * j + 128] = self.slots[3, j]

    def drain(self):
        for stage in range(4):
            @pl.loop(1, 4)
            def _(d):
                self.copy(stage, d).wait_send()


def transpose_into(src, dst):
    @pl.loop(0, 16)
    def _(i):
        cols = src[:, pl.ds(pl.multiple_of(i * 256, 256), 256)]
        dst[i // 4, i % 4] = cols.T.reshape(4, 64, src.shape[0])


def greet(where):
    barrier = pltpu.get_barrier_semaphore()
    for dim in "zyx":
        for shift in (1, 2, 3):
            pl.semaphore_signal(
                barrier, inc=1, device_id=peer(where, dim, shift), device_id_type=MESH
            )
    pl.semaphore_wait(barrier, 9)


def part_scratch():
    shapes = []
    for widths in WIDTHS:
        for width in widths:
            for stage in range(3):
                shapes.append(pltpu.VMEM((6, ROWS[stage], width), SENT[stage]))
                shapes.append(pltpu.VMEM((6, ROWS[stage], width), SENT[stage]))
                if stage < 2:
                    shapes.append(pltpu.VMEM((ROWS[stage] // 32, 64, width), F32))
            shapes.append(pltpu.SemaphoreType.DMA((18,)))
            shapes.append(pltpu.SemaphoreType.DMA((18,)))
    return shapes


def take_parts(where, r, lhs_t, rhs, out, pool):
    parts, off = [], 0
    for p, width in enumerate(WIDTHS[r]):
        bufs = []
        for stage in range(3):
            send, recv = next(pool), next(pool)
            bufs.append((send, recv, next(pool) if stage < 2 else None))
        sems = (next(pool), next(pool))
        parts.append(Part(where, p, lhs_t, rhs, (off, width), out, bufs, sems))
        off += width
    return parts


def wgrad_kernel(feat, cot, act, value_low, gate_low, small,
                 value_out, gate_out, out_out, small_out, feat_t, cot_t,
                 cols, slots, sums, small_ssem, small_rsem, *pool):
    where = coords()
    greet(where)
    pool = iter(pool)
    tiny = Small(where, small, cols, slots, sums, small_out, (small_ssem, small_rsem))
    tiny.send(0)
    transpose_into(cot, cot_t)
    rounds = [
        take_parts(where, 0, cot_t, act, out_out, pool),
        take_parts(where, 1, feat_t, value_low, value_out, pool),
        take_parts(where, 2, feat_t, gate_low, gate_out, pool),
    ]

    def run(name, r, stage):
        for part in rounds[r]:
            getattr(part, name)(stage)

    run("first", 0, 0)
    transpose_into(feat, feat_t)
    run("first", 1, 0)
    run("second", 0, 0)
    run("first", 2, 0)
    run("second", 1, 0)
    run("second", 2, 0)
    tiny.collect(0)
    tiny.send(1)
    run("third", 0, 0)
    run("first", 0, 1)
    tiny.collect(1)
    tiny.send(2)
    run("third", 1, 0)
    run("first", 1, 1)
    run("second", 0, 1)
    run("third", 2, 0)
    run("first", 2, 1)
    tiny.collect(2)
    tiny.send(3)
    run("third", 0, 1)
    run("first", 0, 2)
    run("second", 1, 1)
    run("second", 2, 1)
    run("third", 1, 1)
    run("first", 1, 2)
    run("second", 0, 2)
    run("third", 2, 1)
    run("first", 2, 2)
    run("second", 1, 2)
    run("second", 2, 2)
    tiny.collect(3)
    for r in range(3):
        run("third", r, 2)
    tiny.drain()
    for parts in rounds:
        for part in parts:
            part.drain()


def weight_grads(feat, cot, act, value_low, gate_low, small):
    shape = jax.ShapeDtypeStruct((64, 512), F32)
    vmem = pl.BlockSpec(memory_space=pltpu.VMEM)
    return pl.pallas_call(
        wgrad_kernel,
        out_shape=(shape, shape, shape, jax.ShapeDtypeStruct((32, 512), F32)),
        in_specs=[vmem] * 6,
        out_specs=(vmem,) * 4,
        scratch_shapes=[
            pltpu.VMEM((4, 4, 4, 64, 512), BF16),
            pltpu.VMEM((4, 4, 4, 64, 512), BF16),
            pltpu.VMEM((4, 32, 128), F32),
            pltpu.VMEM((4, 4, 32, 128), F32),
            pltpu.VMEM((3, 32, 128), F32),
            pltpu.SemaphoreType.DMA((16,)),
            pltpu.SemaphoreType.DMA((16,)),
            *part_scratch(),
        ],
        compiler_params=pltpu.CompilerParams(
            collective_id=0, has_side_effects=True, vmem_limit_bytes=64 * 1024 * 1024 - 65536
        ),
    )(feat, cot, act, value_low, gate_low, small)


def in_one_piece(arrays, axis, dim, along):
    ends, at = ([], 0)
    for a in arrays[:-1]:
        at += a.shape[along]
        ends.append(at)
    both = jnp.concatenate(arrays, axis=along)
    return tuple(jnp.split(lax.all_gather(both, axis, axis=dim, tiled=True), ends, axis=along))


def with_halo(block, sides, width):
    for axis, dim in sides:
        count = lax.axis_size(axis)
        forward = [(i, i + 1) for i in range(count - 1)]
        backward = [(target, source) for source, target in forward]
        low = lax.ppermute(
            lax.slice_in_dim(block, block.shape[dim] - width, None, axis=dim), axis, forward
        )
        high = lax.ppermute(lax.slice_in_dim(block, 0, width, axis=dim), axis, backward)
        block = jnp.concatenate([low, block, high], axis=dim)
    return block


def from_everyone(x, axis):
    devices = lax.axis_size(axis)
    return lax.all_to_all(jnp.broadcast_to(x[None], (devices, *x.shape)), axis, 0, 0, tiled=True)


def of_everyone(x, axis):
    return from_everyone(x, axis).sum(axis=0)


def packed_total(arrays, axis):
    vector, at, finished = (jnp.concatenate([a.reshape(-1) for a in arrays]), 0, [])
    running = of_everyone(vector, axis)
    for a in arrays:
        finished.append(running[at : at + a.size].reshape(a.shape))
        at += a.size
    return tuple(finished)


def on_device(features, weight_value, weight_gate, weight_out, conv_taps, norm_gain, out_grad):
    whole_inputs, whole_cotangent = in_one_piece((features, out_grad), "tp", 1, 0)
    value_half = jnp.dot(whole_inputs, weight_value, preferred_element_type=jnp.float32).astype(
        jnp.bfloat16
    )
    gate_half = jnp.dot(whole_inputs, weight_gate, preferred_element_type=jnp.float32).astype(
        jnp.bfloat16
    )
    value_half, gate_half = lax.optimization_barrier((value_half, gate_half))
    value_pre = value_half.astype(jnp.float32)
    gate_pre = gate_half.astype(jnp.float32)
    gate_sig = jax.nn.sigmoid(gate_pre)
    mixed_half = lax.optimization_barrier((value_pre * gate_sig).astype(jnp.bfloat16))
    tap_count = conv_taps.shape[0]
    half_width = tap_count // 2
    row_count = mixed_half.shape[0]
    channels = mixed_half.shape[1] * lax.axis_size("tp")
    extended = with_halo(mixed_half, (("sp", 0),), half_width).astype(jnp.float32)
    conv_out = jnp.zeros(mixed_half.shape, jnp.float32)
    for offset in range(tap_count):
        conv_out = conv_out + conv_taps[offset] * extended[offset : offset + row_count]
    row_sum, row_square = packed_total(
        (jnp.sum(conv_out, axis=-1), jnp.sum(conv_out * conv_out, axis=-1)), "tp"
    )
    mean_row = row_sum[:, None] / channels
    var_row = row_square[:, None] / channels - mean_row * mean_row
    inv_std = lax.rsqrt(var_row + NORM_EPS)
    normed = (conv_out - mean_row) * inv_std
    pre_act = normed * norm_gain
    act_sig = jax.nn.sigmoid(pre_act)
    act_half = (pre_act * act_sig).astype(jnp.bfloat16)
    act_grad = jnp.dot(whole_cotangent, weight_out, preferred_element_type=jnp.float32)
    pre_grad = act_grad * act_sig * (1.0 + pre_act * (1.0 - act_sig))
    gain_part = jnp.sum(pre_grad * normed, axis=0)
    norm_grad = pre_grad * norm_gain
    first_sum, second_sum = packed_total(
        (jnp.sum(norm_grad, axis=-1), jnp.sum(norm_grad * normed, axis=-1)), "tp"
    )
    first_mom = first_sum[:, None] / channels
    second_mom = second_sum[:, None] / channels
    conv_grad = inv_std * (norm_grad - first_mom - normed * second_mom)
    grad_ext = with_halo(conv_grad, (("sp", 0),), half_width)
    mixed_grad = jnp.zeros(conv_grad.shape, jnp.float32)
    taps_rows = []
    for offset in range(tap_count):
        begin = 2 * half_width - offset
        mixed_grad = mixed_grad + conv_taps[offset] * grad_ext[begin : begin + row_count]
        taps_rows.append(jnp.sum(conv_grad * extended[offset : offset + row_count], axis=0))
    value_grad = mixed_grad * gate_sig
    gate_grad = mixed_grad * value_pre * gate_sig * (1.0 - gate_sig)
    value_low = value_grad.astype(jnp.bfloat16)
    gate_low = gate_grad.astype(jnp.bfloat16)
    small = jnp.concatenate([jnp.stack(taps_rows), gain_part[None]], axis=0)
    value_wgrad, gate_wgrad, out_wgrad, small = weight_grads(
        whole_inputs, whole_cotangent, act_half, value_low, gate_low, small
    )
    taps_grad, gain_grad = small[:tap_count], small[tap_count]
    return (value_grad, gate_grad, value_wgrad, gate_wgrad, out_wgrad, taps_grad, gain_grad)


def solution(mesh):
    return jax.shard_map(
        on_device,
        mesh=mesh,
        in_specs=(
            P(SP, "tp"),
            P(None, "tp"),
            P(None, "tp"),
            P(None, "tp"),
            P(None, "tp"),
            P("tp"),
            P(SP, "tp"),
        ),
        out_specs=(
            P(SP, "tp"),
            P(SP, "tp"),
            P(SP, "tp"),
            P(SP, "tp"),
            P(SP, "tp"),
            P(None, "tp"),
            P("tp"),
        ),
        check_vma=False,
    )
```

```python
import functools

import jax
import jax.numpy as jnp
from jax import lax
from jax.experimental import pallas as pl
from jax.experimental.pallas import tpu as pltpu
from jax.sharding import PartitionSpec as P

SP = "sp"
MESH = pl.DeviceIdType.MESH
BF16 = jnp.bfloat16
F32 = jnp.float32

NORM_EPS = 1e-05

WIDTHS = ((128, 128, 256), (256, 128, 128), (128, 256, 128))
ORDERS = ("xzy", "yxz", "zyx")
ROWS = (512, 128, 32)
SENT = (BF16, BF16, F32)


def coords():
    sp = lax.axis_index("sp")
    return {"z": sp // 16, "y": (sp // 4) % 4, "x": sp % 4}


def peer(where, dim, shift):
    to = dict(where)
    to[dim] = (where[dim] + shift + 4) % 4
    return (to["z"] * 16 + to["y"] * 4 + to["x"], lax.axis_index("tp"))


def remote(src, dst, ssem, rsem, device):
    return pltpu.make_async_remote_copy(
        src_ref=src, dst_ref=dst, send_sem=ssem, recv_sem=rsem,
        device_id=device, device_id_type=MESH,
    )


class Part:
    def __init__(self, where, p, lhs_t, rhs, cols, out, bufs, sems):
        self.where, self.p, self.lhs_t, self.rhs = where, p, lhs_t, rhs
        self.cols, self.out, self.bufs, self.sems = cols, out, bufs, sems

    def source(self, stage, h, j):
        off, width = self.cols
        if stage == 0:
            if self.p == 0:
                rows = self.lhs_t[pl.ds(2 * h, 2), :, j]
            elif self.p == 1:
                rows = self.lhs_t[:, j, pl.ds(2 * h, 2)]
            else:
                rows = self.lhs_t[j, pl.ds(2 * h, 2)]
            rows = rows.reshape(512, rows.shape[-1])
            return jnp.dot(rows, self.rhs[:, off : off + width], preferred_element_type=F32)
        held = self.bufs[stage - 1][2]
        if stage == 1:
            if self.p == 1:
                at = (j // 2) * 8 + j % 2
                two = [held[at + 2 * (2 * h + i)] for i in range(2)]
                return jnp.concatenate(two, axis=0)
            return held[pl.ds(4 * j + 2 * h, 2)].reshape(128, width)
        return held[j, pl.ds(pl.multiple_of(h * 32, 32), 32)]

    def place(self, stage, h, value):
        off, width = self.cols
        if stage == 2:
            self.out[pl.ds(pl.multiple_of(h * 32, 32), 32), off : off + width] = value
            return
        held = self.bufs[stage][2]
        count = ROWS[stage] // 64
        held[pl.ds(count * h, count)] = value.reshape(count, 64, width)

    def copy(self, stage, slot, sign):
        send, recv, _ = self.bufs[stage]
        ssem, rsem = self.sems
        at = stage * 6 + slot
        dim = ORDERS[self.p][stage]
        return remote(
            send.at[slot], recv.at[slot], ssem.at[at], rsem.at[at],
            peer(self.where, dim, sign),
        )

    def first(self, stage):
        m = self.where[ORDERS[self.p][stage]]
        send = self.bufs[stage][0]

        @pl.loop(0, 4)
        def _(i):
            sign = 1 - 2 * (i % 2)
            h = ((i + 1) // 2) % 2
            j = (m + 6 - (i // 2) * sign) % 4
            send[i] = self.source(stage, h, j).astype(SENT[stage])
            self.copy(stage, i, sign).start()

    def second(self, stage):
        m = self.where[ORDERS[self.p][stage]]
        send, recv, _ = self.bufs[stage]

        @pl.loop(0, 2)
        def _(k):
            sign = 1 - 2 * k
            self.copy(stage, k, sign).wait_recv()
            mine = self.source(stage, k, (m + 4 + sign) % 4)
            send[4 + k] = (mine + recv[k].astype(F32)).astype(SENT[stage])
            self.copy(stage, 4 + k, sign).start()

    def third(self, stage):
        m = self.where[ORDERS[self.p][stage]]
        recv = self.bufs[stage][1]

        @pl.loop(0, 2)
        def _(h):
            mine = self.source(stage, h, m)
            self.copy(stage, 3 - h, 1).wait_recv()
            self.copy(stage, 4 + h, 1).wait_recv()
            total = mine + recv[3 - h].astype(F32) + recv[4 + h].astype(F32)
            self.place(stage, h, total)

    def drain(self, stage):
        @pl.loop(0, 6)
        def _(slot):
            self.copy(stage, slot, 1).wait_send()


class Small:
    def __init__(self, where, cols, slots, sums, out, sems):
        self.where, self.cols, self.slots = where, cols, slots
        self.sums, self.out, self.sems = sums, out, sems

    def copy(self, stage, d):
        dim = "xyzx"[stage]
        mine = self.where[dim]
        ssem, rsem = self.sems
        src = self.cols.at[(mine + d) % 4] if stage == 0 else self.sums.at[stage - 1]
        at = stage * 4 + d
        return remote(src, self.slots.at[stage, mine], ssem.at[at], rsem.at[at],
                      peer(self.where, dim, d))

    def send(self, stage):
        mine = self.where["xyzx"[stage]]
        if stage == 0:
            self.slots[0, mine] = self.cols[mine]
        else:
            self.slots[stage, mine] = self.sums[stage - 1]

        @pl.loop(1, 4)
        def _(d):
            self.copy(stage, d).start()

    def collect(self, stage):
        @pl.loop(1, 4)
        def _(d):
            self.copy(stage, d).wait_recv()

        if stage < 3:
            a, b, c, d = [self.slots[stage, j] for j in range(4)]
            self.sums[stage] = (a + b) + (c + d)
        else:
            for j in range(4):
                self.out[:, 128 * j : 128 * j + 128] = self.slots[3, j]

    def drain(self):
        for stage in range(4):
            @pl.loop(1, 4)
            def _(d):
                self.copy(stage, d).wait_send()


def greet(where):
    barrier = pltpu.get_barrier_semaphore()
    for to in others(where):
        pl.semaphore_signal(barrier, inc=1, device_id=to, device_id_type=MESH)
    pl.semaphore_wait(barrier, 12)


def partner():
    return (lax.axis_index("sp"), 1 - lax.axis_index("tp"))


def along(shift):
    return ((lax.axis_index("sp") + 64 + shift) % 64, lax.axis_index("tp"))


def others(where):
    near = [peer(where, dim, shift) for dim in "zyx" for shift in (1, 2, 3)]
    return near + [along(-1), along(1), partner()]


AGAIN = {(2, 0): (0, 0), (2, 1): (0, 2), (2, 2): (0, 1)}


def part_scratch():
    shapes = []
    for r, widths in enumerate(WIDTHS):
        for p, width in enumerate(widths):
            for stage in range(3):
                shape = pltpu.VMEM((6, ROWS[stage], width), SENT[stage])
                shapes.append(shape)
                if (r, p) not in AGAIN:
                    shapes.append(shape)
                if stage < 2:
                    shapes.append(pltpu.VMEM((ROWS[stage] // 32, 64, width), F32))
            shapes.append(pltpu.SemaphoreType.DMA((18,)))
            shapes.append(pltpu.SemaphoreType.DMA((18,)))
    return shapes


def take_parts(where, r, lhs_t, rhs, out, pool, earlier):
    parts, off = [], 0
    for p, width in enumerate(WIDTHS[r]):
        bufs = []
        for stage in range(3):
            recv = next(pool)
            if (r, p) in AGAIN:
                r0, p0 = AGAIN[(r, p)]
                send = earlier[r0][p0].bufs[stage][0]
            else:
                send = next(pool)
            bufs.append((send, recv, next(pool) if stage < 2 else None))
        sems = (next(pool), next(pool))
        parts.append(Part(where, p, lhs_t, rhs, (off, width), out, bufs, sems))
        off += width
    return parts


def flip(src, dst, h, k):
    for q in range(2):
        at = pl.multiple_of(k * 512 + q * 256, 256)
        cols = src[h, :, pl.ds(at, 256)]
        dst[h * 2 + k // 2, (k % 2) * 2 + q] = cols.T.reshape(4, 64, 512)


def lane_sum(a):
    return jnp.sum(a, axis=-1, keepdims=True)


def fold(a):
    return jnp.sum(a.reshape(-1, 8, 128), axis=0)


def whole_kernel(
    feat_hbm, wv_hbm, wg_hbm, wo_hbm, taps_in, gain_in, cot_hbm,
    vgrad_hbm, ggrad_hbm, value_out, gate_out, out_out, small_out,
    feat, cot, feat_t, cot_t, wbuf, wobuf, acc0, acc1, acc2, vhalf, ghalf,
    ext, gext, taps, gains, act, vlow, glow, edges, edges_in, gedges, gedges_in,
    stats, stats_in, inv_rows, cols, slots, sums,
    w_sem, wo_sem, f_sem, f_ssem, f_rsem, c_sem, c_ssem, c_rsem,
    e_ssem, e_rsem, s_ssem, s_rsem, o_sem, small_ssem, small_rsem, *pool,
):
    where = coords()
    sp, tp = lax.axis_index("sp"), lax.axis_index("tp")
    pool = iter(pool)
    tiny = Small(where, cols, slots, sums, small_out, (small_ssem, small_rsem))
    out_parts = take_parts(where, 0, cot_t, act, out_out, pool, ())
    value_parts = take_parts(where, 1, feat_t, vlow, value_out, pool, ())
    gate_parts = take_parts(where, 2, feat_t, glow, gate_out, pool, (out_parts,))

    def run(name, parts, stage):
        for part in parts:
            getattr(part, name)(stage)

    def half_of(k):
        return (tp + k // 4) % 2

    def w_loads(k):
        row = pl.multiple_of(half_of(k) * 2048 + (k % 4) * 512, 512)
        slot = k % 3
        return [
            pltpu.make_async_copy(w.at[pl.ds(row, 512)], wbuf.at[slot, i], w_sem.at[slot, i])
            for i, w in enumerate((wv_hbm, wg_hbm))
        ]

    def wo_load(k):
        row = pl.multiple_of(half_of(k) * 2048 + (k % 4) * 512, 512)
        slot = k % 3
        return pltpu.make_async_copy(wo_hbm.at[pl.ds(row, 512)], wobuf.at[slot], wo_sem.at[slot])

    def cut(k):
        return pl.ds(pl.multiple_of(k * 512, 512), 512)

    def own(src, dst, sem, k):
        return pltpu.make_async_copy(src.at[:, cut(k)], dst.at[tp, :, cut(k)], sem.at[k])

    def give(src, dst, ssem, rsem, k):
        return remote(
            src.at[:, cut(k)], dst.at[tp, :, cut(k)], ssem.at[k], rsem.at[k], partner()
        )

    for k in range(2):
        own(feat_hbm, feat, f_sem, k).start()
        for c in w_loads(k):
            c.start()
    greet(where)
    for k in range(4):
        give(feat_hbm, feat, f_ssem, f_rsem, k).start()
    for k in range(2, 4):
        own(feat_hbm, feat, f_sem, k).start()
    for c in w_loads(2):
        c.start()
    for k in range(4):
        give(cot_hbm, cot, c_ssem, c_rsem, k).start()
    for k in range(4):
        own(cot_hbm, cot, c_sem, k).start()
    for k in range(3):
        wo_load(k).start()

    acc0[...] = jnp.zeros_like(acc0)
    acc1[...] = jnp.zeros_like(acc1)
    acc2[...] = jnp.zeros_like(acc2)
    for c in range(4):
        taps[c, 0:31] = taps_in[:, 128 * c : 128 * c + 128]
        gains[c] = jnp.broadcast_to(gain_in[:, 128 * c : 128 * c + 128], (8, 128))

    def add_dot(acc, x, w):
        for c in range(2):
            got = jnp.dot(x, w[:, 256 * c : 256 * c + 256], preferred_element_type=F32)
            acc[2 * c] += got[:, :128]
            acc[2 * c + 1] += got[:, 128:]

    def project(lo, arrived):
        @pl.loop(lo, lo + 4)
        def _(k):
            for c in w_loads(k):
                c.wait()
            arrived(k - lo)
            x = feat[half_of(k), :, cut(k % 4)]
            for i, acc in enumerate((acc0, acc1)):
                add_dot(acc, x, wbuf[k % 3, i])

            @pl.when(k + 3 < 8)
            def _():
                for c in w_loads(k + 3):
                    c.start()

    project(0, lambda k: own(feat_hbm, feat, f_sem, k).wait())
    project(4, lambda k: give(feat_hbm, feat, f_ssem, f_rsem, k).wait_recv())

    def gate_rows(at):
        kept = []
        for c in range(4):
            value = acc0[c, pl.ds(at, 32)].astype(BF16)
            gate = acc1[c, pl.ds(at, 32)].astype(BF16)
            vhalf[c, pl.ds(at, 32)] = value
            ghalf[c, pl.ds(at, 32)] = gate
            sig = jax.nn.sigmoid(gate.astype(F32))
            mixed = (value.astype(F32) * sig).astype(BF16)
            ext[c, pl.ds(at + 16, 32)] = mixed.astype(F32)
            kept.append(mixed)
        return kept

    def edge(send, recv, i, at):
        return remote(send.at[i], recv.at[i], e_ssem.at[at + i], e_rsem.at[at + i],
                      along(2 * i - 1))

    for i, kept in enumerate((gate_rows(0), gate_rows(480))):
        for c in range(4):
            edges[i, c] = kept[c][16 * i : 16 * i + 16]
    for i in range(2):
        edge(edges, edges_in, i, 0).start()

    @pl.loop(1, 15)
    def _(b):
        gate_rows(pl.multiple_of(b * 32, 32))

    def cot_step(lo, arrived):
        @pl.loop(lo, lo + 4)
        def _(k):
            wo_load(k).wait()
            arrived(k - lo)
            h = half_of(k)
            add_dot(acc2, cot[h, :, cut(k % 4)], wobuf[k % 3])
            flip(cot, cot_t, h, k % 4)

            @pl.when(k + 3 < 8)
            def _():
                wo_load(k + 3).start()

    cot_step(0, lambda k: own(cot_hbm, cot, c_sem, k).wait())
    cot_step(4, lambda k: give(cot_hbm, cot, c_ssem, c_rsem, k).wait_recv())

    def fill(buf, got, i):
        inside = sp > 0 if i == 0 else sp < 63
        for c in range(4):
            rows = got[1 - i, c].astype(F32)
            buf[c, 528 * i : 528 * i + 16] = jnp.where(inside, rows, 0.0)

    for i in range(2):
        edge(edges, edges_in, 1 - i, 0).wait_recv()
        fill(ext, edges_in, i)

    def conv(buf, c, at, first, step):
        total = jnp.zeros((64, 128), F32)
        for k in range(31):
            rows = buf[c, pl.ds(at + (first + step * k), 64)]
            total = total + taps[c, k : k + 1] * rows
        return total

    def share(n):
        return remote(stats.at[n], stats_in.at[n], s_ssem.at[n], s_rsem.at[n], partner())

    @pl.loop(0, 8)
    def _(b):
        at = pl.multiple_of(b * 64, 64)
        zero = jnp.zeros((64, 128), F32)

        @pl.loop(0, 4, init_carry=(zero, zero))
        def totals(c, carry):
            got = conv(ext, c, at, 1, 1)
            acc0[c, pl.ds(at, 64)] = got
            return carry[0] + got, carry[1] + got * got

        stats[0, 0, pl.ds(at, 64)] = totals[0]
        stats[0, 1, pl.ds(at, 64)] = totals[1]

    share(0).start()

    @pl.loop(0, 4)
    def _(k):
        flip(feat, feat_t, tp, k)

    share(0).wait_recv()

    none = jnp.zeros((8, 128), F32)

    @pl.loop(0, 16, init_carry=(none,) * 4)
    def gain_sums(b, carry):
        at = pl.multiple_of(b * 32, 32)
        rows = pl.ds(at, 32)
        mean = lane_sum(stats[0, 0, rows] + stats_in[0, 0, rows]) / 1024
        square = lane_sum(stats[0, 1, rows] + stats_in[0, 1, rows]) / 1024
        inv = lax.rsqrt(square - mean * mean + NORM_EPS)
        inv_rows[rows] = jnp.broadcast_to(inv, (32, 128))
        first = jnp.zeros((32, 128), F32)
        second = jnp.zeros((32, 128), F32)
        carried = []
        for c in range(4):
            gain = gains[c, 0:1]
            normed = (acc0[c, rows] - mean) * inv
            pre = normed * gain
            sig = jax.nn.sigmoid(pre)
            act[rows, 128 * c : 128 * c + 128] = (pre * sig).astype(BF16)
            grad = acc2[c, rows] * sig * (1.0 + pre * (1.0 - sig))
            carried.append(carry[c] + fold(grad * normed))
            ngrad = grad * gain
            acc0[c, rows] = normed
            acc1[c, rows] = ngrad
            first = first + ngrad
            second = second + ngrad * normed
        stats[1, 0, rows] = first
        stats[1, 1, rows] = second
        return tuple(carried)

    share(1).start()
    for c in range(4):
        cols[c, 31:32] = jnp.sum(gain_sums[c], axis=0, keepdims=True)
    run("first", out_parts, 0)
    share(1).wait_recv()

    def conv_grad(at):
        rows = pl.ds(at, 32)
        m1 = lane_sum(stats[1, 0, rows] + stats_in[1, 0, rows]) / 1024
        m2 = lane_sum(stats[1, 1, rows] + stats_in[1, 1, rows]) / 1024
        kept = []
        for c in range(4):
            got = inv_rows[rows] * (acc1[c, rows] - m1 - acc0[c, rows] * m2)
            gext[c, pl.ds(at + 16, 32)] = got
            kept.append(got)
        return kept

    for i, kept in enumerate((conv_grad(0), conv_grad(480))):
        for c in range(4):
            gedges[i, c] = kept[c][16 * i : 16 * i + 16]
    for i in range(2):
        edge(gedges, gedges_in, i, 2).start()

    @pl.loop(1, 15)
    def _(b):
        conv_grad(pl.multiple_of(b * 32, 32))

    run("second", out_parts, 0)

    @pl.loop(0, 4)
    def _(c):
        @pl.loop(0, 64, init_carry=(none,) * 31)
        def tap_sums(b, carry):
            at = pl.multiple_of(b * 8, 8)
            grad = gext[c, pl.ds(at + 16, 8)]
            return tuple(
                carry[k] + grad * ext[c, pl.ds(at + (k + 1), 8)] for k in range(31)
            )

        for k in range(31):
            cols[c, k : k + 1] = jnp.sum(tap_sums[k], axis=0, keepdims=True)

    tiny.send(0)

    @pl.loop(0, 4)
    def _(k):
        flip(feat, feat_t, 1 - tp, k)

    for i in range(2):
        edge(gedges, gedges_in, 1 - i, 2).wait_recv()
        fill(gext, gedges_in, i)

    @pl.loop(0, 8)
    def _(b):
        at = pl.multiple_of(b * 64, 64)
        rows = pl.ds(at, 64)

        @pl.loop(0, 4)
        def _(c):
            mixed_grad = conv(gext, c, at, 31, -1)
            value = vhalf[c, rows].astype(F32)
            sig = jax.nn.sigmoid(ghalf[c, rows].astype(F32))
            vgrad = mixed_grad * sig
            ggrad = mixed_grad * value * sig * (1.0 - sig)
            acc0[c, rows] = vgrad
            acc1[c, rows] = ggrad
            lanes = pl.ds(pl.multiple_of(c * 128, 128), 128)
            vlow[rows, lanes] = vgrad.astype(BF16)
            glow[rows, lanes] = ggrad.astype(BF16)

    def store(i, c):
        src, dst = ((acc0, vgrad_hbm), (acc1, ggrad_hbm))[i]
        return pltpu.make_async_copy(
            src.at[c], dst.at[:, 128 * c : 128 * c + 128], o_sem.at[i, c]
        )

    for i in range(2):
        for c in range(4):
            store(i, c).start()

    run("first", value_parts, 0)
    for part in out_parts:
        part.drain(0)
    run("first", gate_parts, 0)
    run("third", out_parts, 0)
    run("first", out_parts, 1)
    tiny.collect(0)
    tiny.send(1)
    run("second", value_parts, 0)
    run("second", gate_parts, 0)
    run("second", out_parts, 1)
    tiny.collect(1)
    tiny.send(2)
    run("third", value_parts, 0)
    run("first", value_parts, 1)
    run("third", out_parts, 1)
    run("first", out_parts, 2)
    tiny.collect(2)
    tiny.send(3)
    for part in out_parts:
        part.drain(1)
    run("third", gate_parts, 0)
    run("first", gate_parts, 1)
    run("second", value_parts, 1)
    run("second", out_parts, 2)
    run("second", gate_parts, 1)
    run("third", out_parts, 2)
    for part in out_parts:
        part.drain(2)
    run("third", value_parts, 1)
    run("first", value_parts, 2)
    run("third", gate_parts, 1)
    run("first", gate_parts, 2)
    run("second", value_parts, 2)
    run("second", gate_parts, 2)
    tiny.collect(3)
    run("third", value_parts, 2)
    run("third", gate_parts, 2)

    tiny.drain()
    for part in (*value_parts, *gate_parts):
        for stage in range(3):
            part.drain(stage)
    for k in range(4):
        give(feat_hbm, feat, f_ssem, f_rsem, k).wait_send()
        give(cot_hbm, cot, c_ssem, c_rsem, k).wait_send()
    for i in range(2):
        edge(edges, edges_in, i, 0).wait_send()
        edge(gedges, gedges_in, i, 2).wait_send()
        share(i).wait_send()
        for c in range(4):
            store(i, c).wait()


def on_device(features, weight_value, weight_gate, weight_out, conv_taps, norm_gain, out_grad):
    grad = jax.ShapeDtypeStruct((512, 512), F32)
    piece = jax.ShapeDtypeStruct((64, 512), F32)
    vmem = pl.BlockSpec(memory_space=pltpu.VMEM)
    hbm = pl.BlockSpec(memory_space=pl.ANY)
    dma = pltpu.SemaphoreType.DMA
    tiles = (4, 512, 128)
    vgrad, ggrad, vw, gw, ow, small = pl.pallas_call(
        whole_kernel,
        out_shape=(grad, grad, piece, piece, piece, jax.ShapeDtypeStruct((32, 512), F32)),
        in_specs=[hbm, hbm, hbm, hbm, vmem, vmem, hbm],
        out_specs=(hbm, hbm, vmem, vmem, vmem, vmem),
        scratch_shapes=[
            pltpu.VMEM((2, 512, 2048), BF16),
            pltpu.VMEM((2, 512, 2048), BF16),
            pltpu.VMEM((4, 4, 4, 64, 512), BF16),
            pltpu.VMEM((4, 4, 4, 64, 512), BF16),
            pltpu.VMEM((3, 2, 512, 512), BF16),
            pltpu.VMEM((3, 512, 512), BF16),
            pltpu.VMEM(tiles, F32),
            pltpu.VMEM(tiles, F32),
            pltpu.VMEM(tiles, F32),
            pltpu.VMEM(tiles, BF16),
            pltpu.VMEM(tiles, BF16),
            pltpu.VMEM((4, 544, 128), F32),
            pltpu.VMEM((4, 544, 128), F32),
            pltpu.VMEM((4, 32, 128), F32),
            pltpu.VMEM((4, 8, 128), F32),
            pltpu.VMEM((512, 512), BF16),
            pltpu.VMEM((512, 512), BF16),
            pltpu.VMEM((512, 512), BF16),
            pltpu.VMEM((2, 4, 16, 128), BF16),
            pltpu.VMEM((2, 4, 16, 128), BF16),
            pltpu.VMEM((2, 4, 16, 128), F32),
            pltpu.VMEM((2, 4, 16, 128), F32),
            pltpu.VMEM((2, 2, 512, 128), F32),
            pltpu.VMEM((2, 2, 512, 128), F32),
            pltpu.VMEM((512, 128), F32),
            pltpu.VMEM((4, 32, 128), F32),
            pltpu.VMEM((4, 4, 32, 128), F32),
            pltpu.VMEM((3, 32, 128), F32),
            dma((3, 2)), dma((3,)),
            dma((4,)), dma((4,)), dma((4,)),
            dma((4,)), dma((4,)), dma((4,)),
            dma((4,)), dma((4,)), dma((2,)), dma((2,)), dma((2, 4)),
            dma((16,)), dma((16,)),
            *part_scratch(),
        ],
        compiler_params=pltpu.CompilerParams(
            collective_id=0, has_side_effects=True, vmem_limit_bytes=64 * 1024 * 1024 - 65536
        ),
    )(features, weight_value, weight_gate, weight_out, conv_taps, norm_gain[None], out_grad)
    return vgrad, ggrad, vw, gw, ow, small[:31], small[31]


def solution(mesh):
    return jax.shard_map(
        on_device,
        mesh=mesh,
        in_specs=(
            P(SP, "tp"), P(None, "tp"), P(None, "tp"), P(None, "tp"),
            P(None, "tp"), P("tp"), P(SP, "tp"),
        ),
        out_specs=(
            P(SP, "tp"), P(SP, "tp"), P(SP, "tp"), P(SP, "tp"), P(SP, "tp"),
            P(None, "tp"), P("tp"),
        ),
        check_vma=False,
    )
```

```python
import functools

import jax
import jax.numpy as jnp
from jax import lax
from jax.experimental import pallas as pl
from jax.experimental.pallas import tpu as pltpu
from jax.sharding import PartitionSpec as P

SP = "sp"
MESH = pl.DeviceIdType.MESH
BF16 = jnp.bfloat16
F32 = jnp.float32

NORM_EPS = 1e-05

WIDTHS = ((128, 128, 256), (256, 128, 128), (128, 256, 128))
ORDERS = ("xzy", "yxz", "zyx")
ROWS = (512, 128, 32)
SENT = (BF16, BF16, F32)


def coords():
    sp = lax.axis_index("sp")
    return {"z": sp // 16, "y": (sp // 4) % 4, "x": sp % 4}


def peer(where, dim, shift):
    to = dict(where)
    to[dim] = (where[dim] + shift + 4) % 4
    return (to["z"] * 16 + to["y"] * 4 + to["x"], lax.axis_index("tp"))


def remote(src, dst, ssem, rsem, device):
    return pltpu.make_async_remote_copy(
        src_ref=src, dst_ref=dst, send_sem=ssem, recv_sem=rsem,
        device_id=device, device_id_type=MESH,
    )


class Part:
    def __init__(self, where, p, lhs_t, rhs, cols, out, bufs, sems, spare):
        self.where, self.p, self.lhs_t, self.rhs = where, p, lhs_t, rhs
        self.cols, self.out, self.bufs, self.sems, self.spare = cols, out, bufs, sems, spare

    def source(self, stage, h, j):
        off, width = self.cols
        if stage == 0:
            if self.p == 0:
                rows = self.lhs_t[pl.ds(2 * h, 2), :, j]
            elif self.p == 1:
                rows = self.lhs_t[:, j, pl.ds(2 * h, 2)]
            else:
                rows = self.lhs_t[j, pl.ds(2 * h, 2)]
            rows = rows.reshape(512, rows.shape[-1])
            return jnp.dot(rows, self.rhs[:, off : off + width], preferred_element_type=F32)
        held = self.bufs[stage - 1][2]
        if stage == 1:
            if self.p == 1:
                at = (j // 2) * 8 + j % 2
                two = [held[at + 2 * (2 * h + i)] for i in range(2)]
                return jnp.concatenate(two, axis=0)
            return held[pl.ds(4 * j + 2 * h, 2)].reshape(128, width)
        return held[j, pl.ds(pl.multiple_of(h * 32, 32), 32)]

    def place(self, stage, h, value):
        off, width = self.cols
        if stage == 2:
            self.out[pl.ds(pl.multiple_of(h * 32, 32), 32), off : off + width] = value
            return
        held = self.bufs[stage][2]
        count = ROWS[stage] // 64
        held[pl.ds(count * h, count)] = value.reshape(count, 64, width)

    def sender(self, stage, slot):
        send = self.bufs[stage][0]
        if send is not None:
            return send.at[slot]
        off, width = self.cols
        lanes = pl.ds(pl.multiple_of((slot % 3) * 512 + off, 128), width)
        return self.spare.at[slot // 3, :, lanes]

    def copy(self, stage, slot, sem, sign):
        recv = self.bufs[stage][1]
        ssem, rsem = self.sems
        return remote(
            recv.at[slot] if isinstance(slot, pl.Slice) else self.sender(stage, slot),
            recv.at[slot], ssem.at[stage], rsem.at[stage * 4 + sem],
            peer(self.where, ORDERS[self.p][stage], sign),
        )

    def first(self, stage):
        m = self.where[ORDERS[self.p][stage]]

        @pl.loop(0, 4)
        def _(i):
            sign = 1 - 2 * (i % 2)
            h = ((i + 1) // 2) % 2
            j = (m + 6 - (i // 2) * sign) % 4
            slot = i + (i // 2) * (2 - 3 * (i % 2))
            self.sender(stage, slot)[...] = self.source(stage, h, j).astype(SENT[stage])
            self.copy(stage, slot, i + (i // 2) * sign, sign).start()

    def second(self, stage):
        m = self.where[ORDERS[self.p][stage]]
        recv = self.bufs[stage][1]

        @pl.loop(0, 2)
        def _(k):
            sign = 1 - 2 * k
            self.copy(stage, k, k, sign).wait_recv()
            mine = self.source(stage, k, (m + 4 + sign) % 4)
            slot = 3 + 2 * k
            total = mine + recv[k].astype(F32)
            self.sender(stage, slot)[...] = total.astype(SENT[stage])
            self.copy(stage, slot, 2 + k, sign).start()

    def third(self, stage):
        m = self.where[ORDERS[self.p][stage]]
        recv = self.bufs[stage][1]

        @pl.loop(0, 2)
        def _(h):
            mine = self.source(stage, h, m)
            self.copy(stage, pl.ds(2 + 2 * h, 2), 2 + h, 1).wait_recv()
            total = mine + recv[2 + 2 * h].astype(F32) + recv[3 + 2 * h].astype(F32)
            self.place(stage, h, total)

    def drain(self, stage):
        self.copy(stage, pl.ds(0, 6), 0, 1).wait_send()


class Small:
    def __init__(self, where, cols, slots, sums, out, sems):
        self.where, self.cols, self.slots = where, cols, slots
        self.sums, self.out, self.sems = sums, out, sems

    def copy(self, stage, d):
        dim = "xyzx"[stage]
        mine = self.where[dim]
        ssem, rsem = self.sems
        src = self.cols.at[(mine + d) % 4] if stage == 0 else self.sums.at[stage - 1]
        at = stage * 4 + d
        return remote(src, self.slots.at[stage, mine], ssem.at[at], rsem.at[at],
                      peer(self.where, dim, d))

    def send(self, stage):
        mine = self.where["xyzx"[stage]]
        if stage == 0:
            self.slots[0, mine] = self.cols[mine]
        else:
            self.slots[stage, mine] = self.sums[stage - 1]

        @pl.loop(1, 4)
        def _(d):
            self.copy(stage, d).start()

    def collect(self, stage):
        @pl.loop(1, 4)
        def _(d):
            self.copy(stage, d).wait_recv()

        if stage < 3:
            a, b, c, d = [self.slots[stage, j] for j in range(4)]
            self.sums[stage] = (a + b) + (c + d)
        else:
            for j in range(4):
                self.out[:, 128 * j : 128 * j + 128] = self.slots[3, j]

    def drain(self):
        for stage in range(4):
            @pl.loop(1, 4)
            def _(d):
                self.copy(stage, d).wait_send()


def greet(where):
    barrier = pltpu.get_barrier_semaphore()
    for to in others(where):
        pl.semaphore_signal(barrier, inc=1, device_id=to, device_id_type=MESH)
    return barrier


def partner():
    return (lax.axis_index("sp"), 1 - lax.axis_index("tp"))


def along(shift):
    return ((lax.axis_index("sp") + 64 + shift) % 64, lax.axis_index("tp"))


def others(where):
    near = [peer(where, dim, shift) for dim in "zyx" for shift in (1, 2, 3)]
    return near + [along(-1), along(1), partner()]


def part_scratch():
    shapes = []
    for r, widths in enumerate(WIDTHS):
        for p, width in enumerate(widths):
            for stage in range(3):
                shape = pltpu.VMEM((6, ROWS[stage], width), SENT[stage])
                shapes.append(shape)
                if (r, stage) != (2, 0):
                    shapes.append(shape)
                if stage < 2:
                    shapes.append(pltpu.VMEM((ROWS[stage] // 32, 64, width), F32))
            shapes.append(pltpu.SemaphoreType.DMA((3,)))
            shapes.append(pltpu.SemaphoreType.DMA((12,)))
    return shapes


def take_parts(where, r, lhs_t, rhs, out, pool, spare=None):
    parts, off = [], 0
    for p, width in enumerate(WIDTHS[r]):
        bufs = []
        for stage in range(3):
            recv = next(pool)
            send = None if (r, stage) == (2, 0) else next(pool)
            bufs.append((send, recv, next(pool) if stage < 2 else None))
        sems = (next(pool), next(pool))
        parts.append(Part(where, p, lhs_t, rhs, (off, width), out, bufs, sems, spare))
        off += width
    return parts


def flip(src, dst, h, k):
    for q in range(2):
        at = pl.multiple_of(k * 512 + q * 256, 256)
        cols = src[h, :, pl.ds(at, 256)]
        dst[h * 2 + k // 2, (k % 2) * 2 + q] = cols.T.reshape(4, 64, 512)


def lane_sum(a):
    return jnp.sum(a, axis=-1, keepdims=True)


def fold(a):
    return jnp.sum(a.reshape(-1, 8, 128), axis=0)


def whole_kernel(
    feat_hbm, wv_hbm, wg_hbm, wo_hbm, taps_in, gain_in, cot_hbm,
    vgrad_hbm, ggrad_hbm, vw_hbm, gw_hbm, ow_hbm, small_hbm,
    value_out, gate_out, out_out, small_out, feat, cot, feat_t, cot_t, wbuf, wobuf, acc0, acc1, acc2, vhalf, ghalf,
    ext, gext, taps, gains, act, vlow, glow, edges, edges_in, gedges, gedges_in,
    stats, stats_in, inv_rows, cols, slots, sums,
    w_sem, wo_sem, f_sem, f_ssem, f_rsem, c_sem, c_ssem, c_rsem,
    e_ssem, e_rsem, s_ssem, s_rsem, o_sem, r_sem, small_ssem, small_rsem, *pool,
):
    where = coords()
    sp, tp = lax.axis_index("sp"), lax.axis_index("tp")
    pool = iter(pool)
    tiny = Small(where, cols, slots, sums, small_out, (small_ssem, small_rsem))
    out_parts = take_parts(where, 0, cot_t, act, out_out, pool)
    value_parts = take_parts(where, 1, feat_t, vlow, value_out, pool)
    gate_parts = take_parts(where, 2, feat_t, glow, gate_out, pool, cot)

    def run(name, parts, stage):
        for part in parts:
            getattr(part, name)(stage)

    def half_of(k):
        return (tp + k // 4) % 2

    def w_loads(k):
        row = pl.multiple_of(half_of(k) * 2048 + (k % 4) * 512, 512)
        slot = k % 3
        return [
            pltpu.make_async_copy(w.at[pl.ds(row, 512)], wbuf.at[slot, i], w_sem.at[slot, i])
            for i, w in enumerate((wv_hbm, wg_hbm))
        ]

    def wo_load(k):
        row = pl.multiple_of(half_of(k) * 2048 + (k % 4) * 512, 512)
        slot = k % 3
        return pltpu.make_async_copy(wo_hbm.at[pl.ds(row, 512)], wobuf.at[slot], wo_sem.at[slot])

    def cut(k):
        return pl.ds(pl.multiple_of(k * 512, 512), 512)

    def own(src, dst, sem, k):
        return pltpu.make_async_copy(src.at[:, cut(k)], dst.at[tp, :, cut(k)], sem.at[k])

    def give(src, dst, ssem, rsem, k):
        return remote(
            src.at[:, cut(k)], dst.at[tp, :, cut(k)], ssem.at[k], rsem.at[k], partner()
        )

    barrier = greet(where)
    for k in range(2):
        for c in w_loads(k):
            c.start()
        own(feat_hbm, feat, f_sem, k).start()
    for c in w_loads(2):
        c.start()
    for k in range(2, 4):
        own(feat_hbm, feat, f_sem, k).start()
    for k in range(4):
        own(cot_hbm, cot, c_sem, k).start()
    for k in range(3):
        wo_load(k).start()

    acc0[...] = jnp.zeros_like(acc0)
    acc1[...] = jnp.zeros_like(acc1)
    acc2[...] = jnp.zeros_like(acc2)
    for c in range(4):
        taps[c, 0:31] = taps_in[:, 128 * c : 128 * c + 128]
        gains[c] = jnp.broadcast_to(gain_in[:, 128 * c : 128 * c + 128], (8, 128))

    def add_dot(acc, x, w):
        for c in range(2):
            got = jnp.dot(x, w[:, 256 * c : 256 * c + 256], preferred_element_type=F32)
            acc[2 * c] += got[:, :128]
            acc[2 * c + 1] += got[:, 128:]

    def project(lo, hi, arrived):
        @pl.loop(lo, hi)
        def _(k):
            for c in w_loads(k):
                c.wait()
            arrived(k % 4)
            x = feat[half_of(k), :, cut(k % 4)]
            for i, acc in enumerate((acc0, acc1)):
                add_dot(acc, x, wbuf[k % 3, i])

            @pl.when(k + 3 < 8)
            def _():
                for c in w_loads(k + 3):
                    c.start()

    def cot_step(lo, hi, arrived):
        @pl.loop(lo, hi)
        def _(k):
            wo_load(k).wait()
            arrived(k % 4)
            h = half_of(k)
            add_dot(acc2, cot[h, :, cut(k % 4)], wobuf[k % 3])
            flip(cot, cot_t, h, k % 4)

            @pl.when(k + 3 < 8)
            def _():
                wo_load(k + 3).start()

    project(0, 2, lambda k: own(feat_hbm, feat, f_sem, k).wait())
    pl.semaphore_wait(barrier, 12)
    for k in range(4):
        give(feat_hbm, feat, f_ssem, f_rsem, k).start()
    for k in range(4):
        give(cot_hbm, cot, c_ssem, c_rsem, k).start()
    project(2, 4, lambda k: own(feat_hbm, feat, f_sem, k).wait())
    cot_step(0, 4, lambda k: own(cot_hbm, cot, c_sem, k).wait())
    project(4, 8, lambda k: give(feat_hbm, feat, f_ssem, f_rsem, k).wait_recv())

    def gate_rows(at):
        kept = []
        for c in range(4):
            value = acc0[c, pl.ds(at, 32)].astype(BF16)
            gate = acc1[c, pl.ds(at, 32)].astype(BF16)
            vhalf[c, pl.ds(at, 32)] = value
            ghalf[c, pl.ds(at, 32)] = gate
            sig = jax.nn.sigmoid(gate.astype(F32))
            mixed = (value.astype(F32) * sig).astype(BF16)
            ext[c, pl.ds(at + 16, 32)] = mixed.astype(F32)
            kept.append(mixed)
        return kept

    def edge(send, recv, i, at):
        return remote(send.at[i], recv.at[i], e_ssem.at[at + i], e_rsem.at[at + i],
                      along(2 * i - 1))

    for i, kept in enumerate((gate_rows(0), gate_rows(480))):
        for c in range(4):
            edges[i, c] = kept[c][16 * i : 16 * i + 16]
    for i in range(2):
        edge(edges, edges_in, i, 0).start()

    @pl.loop(1, 15)
    def _(b):
        gate_rows(pl.multiple_of(b * 32, 32))

    cot_step(4, 8, lambda k: give(cot_hbm, cot, c_ssem, c_rsem, k).wait_recv())

    def fill(buf, got, i):
        inside = sp > 0 if i == 0 else sp < 63
        for c in range(4):
            rows = got[1 - i, c].astype(F32)
            buf[c, 528 * i : 528 * i + 16] = jnp.where(inside, rows, 0.0)

    for i in range(2):
        edge(edges, edges_in, 1 - i, 0).wait_recv()
        fill(ext, edges_in, i)

    def conv(buf, c, at, first, step):
        total = jnp.zeros((64, 128), F32)
        for k in range(31):
            rows = buf[c, pl.ds(at + (first + step * k), 64)]
            total = total + taps[c, k : k + 1] * rows
        return total

    def share(n):
        return remote(stats.at[n], stats_in.at[n], s_ssem.at[n], s_rsem.at[n], partner())

    @pl.loop(0, 8)
    def _(b):
        at = pl.multiple_of(b * 64, 64)
        zero = jnp.zeros((64, 128), F32)

        @pl.loop(0, 4, init_carry=(zero, zero))
        def totals(c, carry):
            got = conv(ext, c, at, 1, 1)
            acc0[c, pl.ds(at, 64)] = got
            return carry[0] + got, carry[1] + got * got

        stats[0, 0, pl.ds(at, 64)] = totals[0]
        stats[0, 1, pl.ds(at, 64)] = totals[1]

    share(0).start()

    @pl.loop(0, 4)
    def _(k):
        flip(feat, feat_t, tp, k)

    share(0).wait_recv()

    none = jnp.zeros((8, 128), F32)

    @pl.loop(0, 16, init_carry=(none,) * 4)
    def gain_sums(b, carry):
        at = pl.multiple_of(b * 32, 32)
        rows = pl.ds(at, 32)
        mean = lane_sum(stats[0, 0, rows] + stats_in[0, 0, rows]) / 1024
        square = lane_sum(stats[0, 1, rows] + stats_in[0, 1, rows]) / 1024
        inv = lax.rsqrt(square - mean * mean + NORM_EPS)
        inv_rows[rows] = jnp.broadcast_to(inv, (32, 128))
        first = jnp.zeros((32, 128), F32)
        second = jnp.zeros((32, 128), F32)
        carried = []
        for c in range(4):
            gain = gains[c, 0:1]
            normed = (acc0[c, rows] - mean) * inv
            pre = normed * gain
            sig = jax.nn.sigmoid(pre)
            act[rows, 128 * c : 128 * c + 128] = (pre * sig).astype(BF16)
            grad = acc2[c, rows] * sig * (1.0 + pre * (1.0 - sig))
            carried.append(carry[c] + fold(grad * normed))
            ngrad = grad * gain
            acc0[c, rows] = normed
            acc1[c, rows] = ngrad
            first = first + ngrad
            second = second + ngrad * normed
        stats[1, 0, rows] = first
        stats[1, 1, rows] = second
        return tuple(carried)

    share(1).start()
    for c in range(4):
        cols[c, 31:32] = jnp.sum(gain_sums[c], axis=0, keepdims=True)
    @pl.loop(0, 4)
    def _(k):
        flip(feat, feat_t, 1 - tp, k)

    share(1).wait_recv()

    def conv_grad(at):
        rows = pl.ds(at, 32)
        m1 = lane_sum(stats[1, 0, rows] + stats_in[1, 0, rows]) / 1024
        m2 = lane_sum(stats[1, 1, rows] + stats_in[1, 1, rows]) / 1024
        kept = []
        for c in range(4):
            got = inv_rows[rows] * (acc1[c, rows] - m1 - acc0[c, rows] * m2)
            gext[c, pl.ds(at + 16, 32)] = got
            kept.append(got)
        return kept

    for i, kept in enumerate((conv_grad(0), conv_grad(480))):
        for c in range(4):
            gedges[i, c] = kept[c][16 * i : 16 * i + 16]
    for i in range(2):
        edge(gedges, gedges_in, i, 2).start()

    run("first", out_parts, 0)

    @pl.loop(1, 15)
    def _(b):
        conv_grad(pl.multiple_of(b * 32, 32))

    for i in range(2):
        edge(gedges, gedges_in, 1 - i, 2).wait_recv()
        fill(gext, gedges_in, i)

    @pl.loop(0, 8)
    def _(b):
        at = pl.multiple_of(b * 64, 64)
        rows = pl.ds(at, 64)

        @pl.loop(0, 4)
        def _(c):
            mixed_grad = conv(gext, c, at, 31, -1)
            value = vhalf[c, rows].astype(F32)
            sig = jax.nn.sigmoid(ghalf[c, rows].astype(F32))
            vgrad = mixed_grad * sig
            ggrad = mixed_grad * value * sig * (1.0 - sig)
            acc0[c, rows] = vgrad
            acc1[c, rows] = ggrad
            lanes = pl.ds(pl.multiple_of(c * 128, 128), 128)
            vlow[rows, lanes] = vgrad.astype(BF16)
            glow[rows, lanes] = ggrad.astype(BF16)

    def store(i, c):
        src, dst = ((acc0, vgrad_hbm), (acc1, ggrad_hbm))[i]
        return pltpu.make_async_copy(
            src.at[c], dst.at[:, 128 * c : 128 * c + 128], o_sem.at[i, c]
        )

    def leave(i):
        src = (value_out, gate_out, out_out, small_out)[i]
        dst = (vw_hbm, gw_hbm, ow_hbm, small_hbm)[i]
        return pltpu.make_async_copy(src, dst, r_sem.at[i])

    for i in range(2):
        for c in range(4):
            store(i, c).start()

    run("first", value_parts, 0)
    run("second", out_parts, 0)
    run("first", gate_parts, 0)
    run("third", out_parts, 0)
    run("first", out_parts, 1)
    @pl.loop(0, 4)
    def _(c):
        @pl.loop(0, 16, init_carry=(none,) * 31)
        def tap_sums(b, carry):
            at = pl.multiple_of(b * 32, 32)
            grad = gext[c, pl.ds(at + 16, 32)]
            return tuple(
                carry[k] + fold(grad * ext[c, pl.ds(at + (k + 1), 32)]) for k in range(31)
            )

        for k in range(31):
            cols[c, k : k + 1] = jnp.sum(tap_sums[k], axis=0, keepdims=True)

    tiny.send(0)

    run("second", value_parts, 0)
    run("second", gate_parts, 0)
    run("second", out_parts, 1)
    run("third", value_parts, 0)
    run("first", value_parts, 1)
    tiny.collect(0)
    tiny.send(1)
    run("third", out_parts, 1)
    run("first", out_parts, 2)
    run("third", gate_parts, 0)
    run("first", gate_parts, 1)
    run("second", value_parts, 1)
    tiny.collect(1)
    tiny.send(2)
    run("second", out_parts, 2)
    run("second", gate_parts, 1)
    run("third", value_parts, 1)
    run("first", value_parts, 2)
    tiny.collect(2)
    tiny.send(3)
    run("third", gate_parts, 1)
    run("first", gate_parts, 2)
    run("third", out_parts, 2)
    leave(2).start()
    run("second", value_parts, 2)
    run("second", gate_parts, 2)
    run("third", value_parts, 2)
    leave(0).start()
    run("third", gate_parts, 2)
    leave(1).start()
    tiny.collect(3)
    leave(3).start()

    tiny.drain()
    for part in (*out_parts, *value_parts, *gate_parts):
        for stage in range(3):
            part.drain(stage)
    for k in range(4):
        give(feat_hbm, feat, f_ssem, f_rsem, k).wait_send()
        give(cot_hbm, cot, c_ssem, c_rsem, k).wait_send()
    for i in range(2):
        edge(edges, edges_in, i, 0).wait_send()
        edge(gedges, gedges_in, i, 2).wait_send()
        share(i).wait_send()
        for c in range(4):
            store(i, c).wait()
    for i in range(4):
        leave(i).wait()


def hand_kernel(vgrad, ggrad, vw, gw, ow, small, vgrad_o, ggrad_o, vw_o, gw_o, ow_o,
                taps_o, gain_o, big, mid, tiny, taps, gain, in_sem, out_sem):
    moves = []
    for i, (src, dst) in enumerate(((vgrad, vgrad_o), (ggrad, ggrad_o))):
        for q in range(4):
            rows = pl.ds(q * 128, 128)
            moves.append((src.at[rows], big.at[i, rows], [(big.at[i, rows], dst.at[rows])]))
    for i, (src, dst) in enumerate(((vw, vw_o), (gw, gw_o), (ow, ow_o))):
        moves.append((src, mid.at[i], [(mid.at[i], dst)]))
    moves.append((small, tiny, [(taps, taps_o), (gain, gain_o)]))
    ins = [
        pltpu.make_async_copy(src, held, in_sem.at[i]) for i, (src, held, _) in enumerate(moves)
    ]
    outs, at = [], 0
    for copy in ins:
        copy.start()
    for copy, (_, _, goes) in zip(ins, moves):
        copy.wait()
        if len(goes) == 2:
            taps[...] = tiny[0:31]
            gain[...] = tiny[31:32]
        for src, dst in goes:
            outs.append(pltpu.make_async_copy(src, dst, out_sem.at[at]))
            outs[-1].start()
            at += 1
    for copy in outs:
        copy.wait()


def on_device(features, weight_value, weight_gate, weight_out, conv_taps, norm_gain, out_grad):
    grad = jax.ShapeDtypeStruct((512, 512), F32)
    piece = jax.ShapeDtypeStruct((64, 512), F32)
    vmem = pl.BlockSpec(memory_space=pltpu.VMEM)
    hbm = pl.BlockSpec(memory_space=pl.ANY)
    dma = pltpu.SemaphoreType.DMA
    tiles = (4, 512, 128)
    vgrad, ggrad, vw, gw, ow, small = pl.pallas_call(
        whole_kernel,
        out_shape=(grad, grad, piece, piece, piece, jax.ShapeDtypeStruct((32, 512), F32)),
        in_specs=[hbm, hbm, hbm, hbm, vmem, vmem, hbm],
        out_specs=(hbm,) * 6,
        scratch_shapes=[
            *[pltpu.VMEM((64, 512), F32)] * 3,
            pltpu.VMEM((32, 512), F32),
            pltpu.VMEM((2, 512, 2048), BF16),
            pltpu.VMEM((2, 512, 2048), BF16),
            pltpu.VMEM((4, 4, 4, 64, 512), BF16),
            pltpu.VMEM((4, 4, 4, 64, 512), BF16),
            pltpu.VMEM((3, 2, 512, 512), BF16),
            pltpu.VMEM((3, 512, 512), BF16),
            pltpu.VMEM(tiles, F32),
            pltpu.VMEM(tiles, F32),
            pltpu.VMEM(tiles, F32),
            pltpu.VMEM(tiles, BF16),
            pltpu.VMEM(tiles, BF16),
            pltpu.VMEM((4, 544, 128), F32),
            pltpu.VMEM((4, 544, 128), F32),
            pltpu.VMEM((4, 32, 128), F32),
            pltpu.VMEM((4, 8, 128), F32),
            pltpu.VMEM((512, 512), BF16),
            pltpu.VMEM((512, 512), BF16),
            pltpu.VMEM((512, 512), BF16),
            pltpu.VMEM((2, 4, 16, 128), BF16),
            pltpu.VMEM((2, 4, 16, 128), BF16),
            pltpu.VMEM((2, 4, 16, 128), F32),
            pltpu.VMEM((2, 4, 16, 128), F32),
            pltpu.VMEM((2, 2, 512, 128), F32),
            pltpu.VMEM((2, 2, 512, 128), F32),
            pltpu.VMEM((512, 128), F32),
            pltpu.VMEM((4, 32, 128), F32),
            pltpu.VMEM((4, 4, 32, 128), F32),
            pltpu.VMEM((3, 32, 128), F32),
            dma((3, 2)), dma((3,)),
            dma((4,)), dma((4,)), dma((4,)),
            dma((4,)), dma((4,)), dma((4,)),
            dma((4,)), dma((4,)), dma((2,)), dma((2,)), dma((2, 4)), dma((4,)),
            dma((16,)), dma((16,)),
            *part_scratch(),
        ],
        compiler_params=pltpu.CompilerParams(
            collective_id=0, has_side_effects=True, vmem_limit_bytes=64 * 1024 * 1024 - 65536
        ),
    )(features, weight_value, weight_gate, weight_out, conv_taps, norm_gain[None], out_grad)
    *rest, gain = pl.pallas_call(
        hand_kernel,
        out_shape=(
            grad, grad, piece, piece, piece,
            jax.ShapeDtypeStruct((31, 512), F32), jax.ShapeDtypeStruct((1, 512), F32),
        ),
        in_specs=[hbm] * 6,
        out_specs=(hbm,) * 7,
        scratch_shapes=[
            pltpu.VMEM((2, 512, 512), F32),
            pltpu.VMEM((3, 64, 512), F32),
            pltpu.VMEM((32, 512), F32),
            pltpu.VMEM((31, 512), F32),
            pltpu.VMEM((1, 512), F32),
            dma((12,)), dma((13,)),
        ],
    )(vgrad, ggrad, vw, gw, ow, small)
    return (*rest, gain[0])


def solution(mesh):
    return jax.shard_map(
        on_device,
        mesh=mesh,
        in_specs=(
            P(SP, "tp"), P(None, "tp"), P(None, "tp"), P(None, "tp"),
            P(None, "tp"), P("tp"), P(SP, "tp"),
        ),
        out_specs=(
            P(SP, "tp"), P(SP, "tp"), P(SP, "tp"), P(SP, "tp"), P(SP, "tp"),
            P(None, "tp"), P("tp"),
        ),
        check_vma=False,
    )
```

```python
import functools

import jax
import jax.numpy as jnp
from jax import lax
from jax.experimental import pallas as pl
from jax.experimental.pallas import tpu as pltpu
from jax.sharding import PartitionSpec as P

SP = "sp"
MESH = pl.DeviceIdType.MESH
BF16 = jnp.bfloat16
F32 = jnp.float32

NORM_EPS = 1e-05

WIDTHS = ((128, 128, 256), (256, 128, 128), (128, 256, 128))
ORDERS = ("xzy", "yxz", "zyx")
ROWS = (512, 128, 32)
SENT = (BF16, BF16, F32)


def coords():
    sp = lax.axis_index("sp")
    return {"z": sp // 16, "y": (sp // 4) % 4, "x": sp % 4}


def peer(where, dim, shift):
    to = dict(where)
    to[dim] = (where[dim] + shift + 4) % 4
    return (to["z"] * 16 + to["y"] * 4 + to["x"], lax.axis_index("tp"))


def remote(src, dst, ssem, rsem, device):
    return pltpu.make_async_remote_copy(
        src_ref=src, dst_ref=dst, send_sem=ssem, recv_sem=rsem,
        device_id=device, device_id_type=MESH,
    )


class Part:
    def __init__(self, where, p, lhs_t, rhs, cols, out, bufs, sems, spare):
        self.where, self.p, self.lhs_t, self.rhs = where, p, lhs_t, rhs
        self.cols, self.out, self.bufs, self.sems, self.spare = cols, out, bufs, sems, spare

    def source(self, stage, h, j):
        off, width = self.cols
        if stage == 0:
            if self.p == 0:
                rows = self.lhs_t[pl.ds(2 * h, 2), :, j]
            elif self.p == 1:
                rows = self.lhs_t[:, j, pl.ds(2 * h, 2)]
            else:
                rows = self.lhs_t[j, pl.ds(2 * h, 2)]
            rows = rows.reshape(512, rows.shape[-1])
            return jnp.dot(rows, self.rhs[:, off : off + width], preferred_element_type=F32)
        held = self.bufs[stage - 1][2]
        if stage == 1:
            if self.p == 1:
                at = (j // 2) * 8 + j % 2
                two = [held[at + 2 * (2 * h + i)] for i in range(2)]
                return jnp.concatenate(two, axis=0)
            return held[pl.ds(4 * j + 2 * h, 2)].reshape(128, width)
        return held[j, pl.ds(pl.multiple_of(h * 32, 32), 32)]

    def place(self, stage, h, value):
        off, width = self.cols
        if stage == 2:
            self.out[pl.ds(pl.multiple_of(h * 32, 32), 32), off : off + width] = value
            return
        held = self.bufs[stage][2]
        count = ROWS[stage] // 64
        held[pl.ds(count * h, count)] = value.reshape(count, 64, width)

    def sender(self, stage, slot):
        send = self.bufs[stage][0]
        if send is not None:
            return send.at[slot]
        off, width = self.cols
        lanes = pl.ds(pl.multiple_of((slot % 3) * 512 + off, 128), width)
        return self.spare.at[slot // 3, :, lanes]

    def copy(self, stage, slot, sem, sign):
        recv = self.bufs[stage][1]
        ssem, rsem = self.sems
        return remote(
            recv.at[slot] if isinstance(slot, pl.Slice) else self.sender(stage, slot),
            recv.at[slot], ssem.at[stage], rsem.at[stage * 4 + sem],
            peer(self.where, ORDERS[self.p][stage], sign),
        )

    def first(self, stage):
        m = self.where[ORDERS[self.p][stage]]

        @pl.loop(0, 4)
        def _(i):
            sign = 1 - 2 * (i % 2)
            h = ((i + 1) // 2) % 2
            j = (m + 6 - (i // 2) * sign) % 4
            slot = i + (i // 2) * (2 - 3 * (i % 2))
            self.sender(stage, slot)[...] = self.source(stage, h, j).astype(SENT[stage])
            self.copy(stage, slot, i + (i // 2) * sign, sign).start()

    def second(self, stage):
        m = self.where[ORDERS[self.p][stage]]
        recv = self.bufs[stage][1]

        @pl.loop(0, 2)
        def _(k):
            sign = 1 - 2 * k
            self.copy(stage, k, k, sign).wait_recv()
            mine = self.source(stage, k, (m + 4 + sign) % 4)
            slot = 3 + 2 * k
            total = mine + recv[k].astype(F32)
            self.sender(stage, slot)[...] = total.astype(SENT[stage])
            self.copy(stage, slot, 2 + k, sign).start()

    def third(self, stage):
        m = self.where[ORDERS[self.p][stage]]
        recv = self.bufs[stage][1]

        @pl.loop(0, 2)
        def _(h):
            mine = self.source(stage, h, m)
            self.copy(stage, pl.ds(2 + 2 * h, 2), 2 + h, 1).wait_recv()
            total = mine + recv[2 + 2 * h].astype(F32) + recv[3 + 2 * h].astype(F32)
            self.place(stage, h, total)

    def drain(self, stage):
        self.copy(stage, pl.ds(0, 6), 0, 1).wait_send()


class Small:
    def __init__(self, where, cols, slots, sums, out, sems):
        self.where, self.cols, self.slots = where, cols, slots
        self.sums, self.out, self.sems = sums, out, sems

    def copy(self, stage, d):
        dim = "xyzx"[stage]
        mine = self.where[dim]
        ssem, rsem = self.sems
        src = self.cols.at[(mine + d) % 4] if stage == 0 else self.sums.at[stage - 1]
        at = stage * 4 + d
        return remote(src, self.slots.at[stage, mine], ssem.at[at], rsem.at[at],
                      peer(self.where, dim, d))

    def send(self, stage):
        mine = self.where["xyzx"[stage]]
        if stage == 0:
            self.slots[0, mine] = self.cols[mine]
        else:
            self.slots[stage, mine] = self.sums[stage - 1]

        @pl.loop(1, 4)
        def _(d):
            self.copy(stage, d).start()

    def collect(self, stage):
        @pl.loop(1, 4)
        def _(d):
            self.copy(stage, d).wait_recv()

        if stage < 3:
            a, b, c, d = [self.slots[stage, j] for j in range(4)]
            self.sums[stage] = (a + b) + (c + d)
        else:
            for j in range(4):
                self.out[:, 128 * j : 128 * j + 128] = self.slots[3, j]

    def drain(self):
        for stage in range(4):
            @pl.loop(1, 4)
            def _(d):
                self.copy(stage, d).wait_send()


def greet(where):
    barrier = pltpu.get_barrier_semaphore()
    for to in others(where):
        pl.semaphore_signal(barrier, inc=1, device_id=to, device_id_type=MESH)
    return barrier


def partner():
    return (lax.axis_index("sp"), 1 - lax.axis_index("tp"))


def along(shift):
    return ((lax.axis_index("sp") + 64 + shift) % 64, lax.axis_index("tp"))


def others(where):
    near = [peer(where, dim, shift) for dim in "zyx" for shift in (1, 2, 3)]
    return near + [along(-1), along(1), partner()]


def part_scratch():
    shapes = []
    for r, widths in enumerate(WIDTHS):
        for p, width in enumerate(widths):
            for stage in range(3):
                shape = pltpu.VMEM((6, ROWS[stage], width), SENT[stage])
                shapes.append(shape)
                if (r, stage) != (2, 0):
                    shapes.append(shape)
                if stage < 2:
                    shapes.append(pltpu.VMEM((ROWS[stage] // 32, 64, width), F32))
            shapes.append(pltpu.SemaphoreType.DMA((3,)))
            shapes.append(pltpu.SemaphoreType.DMA((12,)))
    return shapes


def take_parts(where, r, lhs_t, rhs, out, pool, spare=None):
    parts, off = [], 0
    for p, width in enumerate(WIDTHS[r]):
        bufs = []
        for stage in range(3):
            recv = next(pool)
            send = None if (r, stage) == (2, 0) else next(pool)
            bufs.append((send, recv, next(pool) if stage < 2 else None))
        sems = (next(pool), next(pool))
        parts.append(Part(where, p, lhs_t, rhs, (off, width), out, bufs, sems, spare))
        off += width
    return parts


def flip(src, dst, h, k):
    for q in range(2):
        at = pl.multiple_of(k * 512 + q * 256, 256)
        cols = src[h, :, pl.ds(at, 256)]
        dst[h * 2 + k // 2, (k % 2) * 2 + q] = cols.T.reshape(4, 64, 512)


def lane_sum(a):
    return jnp.sum(a, axis=-1, keepdims=True)


def fold(a):
    return jnp.sum(a.reshape(-1, 8, 128), axis=0)


def whole_kernel(
    feat_hbm, wv_hbm, wg_hbm, wo_hbm, taps_in, gain_in, cot_hbm,
    vgrad_hbm, ggrad_hbm, vw_hbm, gw_hbm, ow_hbm, small_hbm,
    value_out, gate_out, out_out, small_out, feat, cot, feat_t, cot_t, wbuf, wobuf, acc0, acc1, acc2, vhalf, ghalf,
    ext, gext, taps, gains, act, vlow, glow, edges, edges_in, gedges, gedges_in,
    stats, stats_in, inv_rows, cols, slots, sums,
    w_sem, wo_sem, f_sem, f_ssem, f_rsem, c_sem, c_ssem, c_rsem,
    e_ssem, e_rsem, s_ssem, s_rsem, o_sem, r_sem, small_ssem, small_rsem, *pool,
):
    where = coords()
    sp, tp = lax.axis_index("sp"), lax.axis_index("tp")
    pool = iter(pool)
    tiny = Small(where, cols, slots, sums, small_out, (small_ssem, small_rsem))
    out_parts = take_parts(where, 0, cot_t, act, out_out, pool)
    value_parts = take_parts(where, 1, feat_t, vlow, value_out, pool)
    gate_parts = take_parts(where, 2, feat_t, glow, gate_out, pool, cot)

    def run(name, parts, stage):
        for part in parts:
            getattr(part, name)(stage)

    def half_of(k):
        return (tp + k // 4) % 2

    def w_loads(k):
        row = pl.multiple_of(half_of(k) * 2048 + (k % 4) * 512, 512)
        slot = k % 3
        return [
            pltpu.make_async_copy(w.at[pl.ds(row, 512)], wbuf.at[slot, i], w_sem.at[slot, i])
            for i, w in enumerate((wv_hbm, wg_hbm))
        ]

    def wo_load(k):
        row = pl.multiple_of(half_of(k) * 2048 + (k % 4) * 512, 512)
        slot = k % 3
        return pltpu.make_async_copy(wo_hbm.at[pl.ds(row, 512)], wobuf.at[slot], wo_sem.at[slot])

    def cut(k):
        return pl.ds(pl.multiple_of(k * 512, 512), 512)

    def own(src, dst, sem, k):
        return pltpu.make_async_copy(src.at[:, cut(k)], dst.at[tp, :, cut(k)], sem.at[k])

    def give(src, dst, ssem, rsem, k):
        return remote(
            src.at[:, cut(k)], dst.at[tp, :, cut(k)], ssem.at[k], rsem.at[k], partner()
        )

    barrier = greet(where)
    for k in range(2):
        for c in w_loads(k):
            c.start()
        own(feat_hbm, feat, f_sem, k).start()
    for c in w_loads(2):
        c.start()
    for k in range(2, 4):
        own(feat_hbm, feat, f_sem, k).start()
    for k in range(4):
        own(cot_hbm, cot, c_sem, k).start()
    for k in range(3):
        wo_load(k).start()

    acc0[...] = jnp.zeros_like(acc0)
    acc1[...] = jnp.zeros_like(acc1)
    acc2[...] = jnp.zeros_like(acc2)
    for c in range(4):
        taps[c, 0:31] = taps_in[:, 128 * c : 128 * c + 128]
        gains[c] = jnp.broadcast_to(gain_in[:, 128 * c : 128 * c + 128], (8, 128))

    def add_dot(acc, x, w):
        for c in range(2):
            got = jnp.dot(x, w[:, 256 * c : 256 * c + 256], preferred_element_type=F32)
            acc[2 * c] += got[:, :128]
            acc[2 * c + 1] += got[:, 128:]

    def project(lo, hi, arrived):
        @pl.loop(lo, hi)
        def _(k):
            for c in w_loads(k):
                c.wait()
            arrived(k % 4)
            x = feat[half_of(k), :, cut(k % 4)]
            for i, acc in enumerate((acc0, acc1)):
                add_dot(acc, x, wbuf[k % 3, i])

            @pl.when(k + 3 < 8)
            def _():
                for c in w_loads(k + 3):
                    c.start()

    def cot_step(lo, hi, arrived):
        @pl.loop(lo, hi)
        def _(k):
            wo_load(k).wait()
            arrived(k % 4)
            h = half_of(k)
            add_dot(acc2, cot[h, :, cut(k % 4)], wobuf[k % 3])
            flip(cot, cot_t, h, k % 4)

            @pl.when(k + 3 < 8)
            def _():
                wo_load(k + 3).start()

    project(0, 2, lambda k: own(feat_hbm, feat, f_sem, k).wait())
    pl.semaphore_wait(barrier, 12)
    for k in range(4):
        give(feat_hbm, feat, f_ssem, f_rsem, k).start()
    for k in range(4):
        give(cot_hbm, cot, c_ssem, c_rsem, k).start()
    project(2, 4, lambda k: own(feat_hbm, feat, f_sem, k).wait())
    cot_step(0, 4, lambda k: own(cot_hbm, cot, c_sem, k).wait())
    project(4, 8, lambda k: give(feat_hbm, feat, f_ssem, f_rsem, k).wait_recv())

    def gate_rows(at):
        kept = []
        for c in range(4):
            value = acc0[c, pl.ds(at, 32)].astype(BF16)
            gate = acc1[c, pl.ds(at, 32)].astype(BF16)
            vhalf[c, pl.ds(at, 32)] = value
            ghalf[c, pl.ds(at, 32)] = gate
            sig = jax.nn.sigmoid(gate.astype(F32))
            mixed = (value.astype(F32) * sig).astype(BF16)
            ext[c, pl.ds(at + 16, 32)] = mixed.astype(F32)
            kept.append(mixed)
        return kept

    def edge(send, recv, i, at):
        return remote(send.at[i], recv.at[i], e_ssem.at[at + i], e_rsem.at[at + i],
                      along(2 * i - 1))

    for i, kept in enumerate((gate_rows(0), gate_rows(480))):
        for c in range(4):
            edges[i, c] = kept[c][16 * i : 16 * i + 16]
    for i in range(2):
        edge(edges, edges_in, i, 0).start()

    @pl.loop(1, 15)
    def _(b):
        gate_rows(pl.multiple_of(b * 32, 32))

    cot_step(4, 8, lambda k: give(cot_hbm, cot, c_ssem, c_rsem, k).wait_recv())

    def fill(buf, got, i):
        inside = sp > 0 if i == 0 else sp < 63
        for c in range(4):
            rows = got[1 - i, c].astype(F32)
            buf[c, 528 * i : 528 * i + 16] = jnp.where(inside, rows, 0.0)

    def conv(buf, c, at, first, step):
        total = jnp.zeros((64, 128), F32)
        for k in range(31):
            rows = buf[c, pl.ds(at + (first + step * k), 64)]
            total = total + taps[c, k : k + 1] * rows
        return total

    def share(n):
        return remote(stats.at[n], stats_in.at[n], s_ssem.at[n], s_rsem.at[n], partner())

    def conv_rows(b):
        at = pl.multiple_of(b * 64, 64)
        zero = jnp.zeros((64, 128), F32)

        @pl.loop(0, 4, init_carry=(zero, zero))
        def totals(c, carry):
            got = conv(ext, c, at, 1, 1)
            acc0[c, pl.ds(at, 64)] = got
            return carry[0] + got, carry[1] + got * got

        stats[0, 0, pl.ds(at, 64)] = totals[0]
        stats[0, 1, pl.ds(at, 64)] = totals[1]

    pl.loop(1, 7)(conv_rows)
    for i in range(2):
        edge(edges, edges_in, 1 - i, 0).wait_recv()
        fill(ext, edges_in, i)

    pl.loop(0, 8, step=7)(conv_rows)
    share(0).start()

    @pl.loop(0, 4)
    def _(k):
        flip(feat, feat_t, tp, k)

    share(0).wait_recv()

    none = jnp.zeros((8, 128), F32)

    @pl.loop(0, 16, init_carry=(none,) * 4)
    def gain_sums(b, carry):
        at = pl.multiple_of(b * 32, 32)
        rows = pl.ds(at, 32)
        mean = lane_sum(stats[0, 0, rows] + stats_in[0, 0, rows]) / 1024
        square = lane_sum(stats[0, 1, rows] + stats_in[0, 1, rows]) / 1024
        inv = lax.rsqrt(square - mean * mean + NORM_EPS)
        inv_rows[rows] = jnp.broadcast_to(inv, (32, 128))
        first = jnp.zeros((32, 128), F32)
        second = jnp.zeros((32, 128), F32)
        carried = []
        for c in range(4):
            gain = gains[c, 0:1]
            normed = (acc0[c, rows] - mean) * inv
            pre = normed * gain
            sig = jax.nn.sigmoid(pre)
            act[rows, 128 * c : 128 * c + 128] = (pre * sig).astype(BF16)
            grad = acc2[c, rows] * sig * (1.0 + pre * (1.0 - sig))
            carried.append(carry[c] + fold(grad * normed))
            ngrad = grad * gain
            acc0[c, rows] = normed
            acc1[c, rows] = ngrad
            first = first + ngrad
            second = second + ngrad * normed
        stats[1, 0, rows] = first
        stats[1, 1, rows] = second
        return tuple(carried)

    share(1).start()
    for c in range(4):
        cols[c, 31:32] = jnp.sum(gain_sums[c], axis=0, keepdims=True)
    run("first", out_parts[2:], 0)
    share(1).wait_recv()

    def conv_grad(at):
        rows = pl.ds(at, 32)
        m1 = lane_sum(stats[1, 0, rows] + stats_in[1, 0, rows]) / 1024
        m2 = lane_sum(stats[1, 1, rows] + stats_in[1, 1, rows]) / 1024
        kept = []
        for c in range(4):
            got = inv_rows[rows] * (acc1[c, rows] - m1 - acc0[c, rows] * m2)
            gext[c, pl.ds(at + 16, 32)] = got
            kept.append(got)
        return kept

    for i, kept in enumerate((conv_grad(0), conv_grad(480))):
        for c in range(4):
            gedges[i, c] = kept[c][16 * i : 16 * i + 16]
    for i in range(2):
        edge(gedges, gedges_in, i, 2).start()

    run("first", out_parts[:2], 0)

    @pl.loop(1, 15)
    def _(b):
        conv_grad(pl.multiple_of(b * 32, 32))

    def grad_rows(b):
        at = pl.multiple_of(b * 64, 64)
        rows = pl.ds(at, 64)

        @pl.loop(0, 4)
        def _(c):
            mixed_grad = conv(gext, c, at, 31, -1)
            value = vhalf[c, rows].astype(F32)
            sig = jax.nn.sigmoid(ghalf[c, rows].astype(F32))
            vgrad = mixed_grad * sig
            ggrad = mixed_grad * value * sig * (1.0 - sig)
            acc0[c, rows] = vgrad
            acc1[c, rows] = ggrad
            lanes = pl.ds(pl.multiple_of(c * 128, 128), 128)
            vlow[rows, lanes] = vgrad.astype(BF16)
            glow[rows, lanes] = ggrad.astype(BF16)

    @pl.loop(0, 4)
    def _(k):
        flip(feat, feat_t, 1 - tp, k)

    pl.loop(1, 7)(grad_rows)
    run("second", out_parts[:2], 0)
    for i in range(2):
        edge(gedges, gedges_in, 1 - i, 2).wait_recv()
        fill(gext, gedges_in, i)

    pl.loop(0, 8, step=7)(grad_rows)

    def store(i, c):
        src, dst = ((acc0, vgrad_hbm), (acc1, ggrad_hbm))[i]
        return pltpu.make_async_copy(
            src.at[c], dst.at[:, 128 * c : 128 * c + 128], o_sem.at[i, c]
        )

    def leave(i):
        src = (value_out, gate_out, out_out, small_out)[i]
        dst = (vw_hbm, gw_hbm, ow_hbm, small_hbm)[i]
        return pltpu.make_async_copy(src, dst, r_sem.at[i])

    for i in range(2):
        for c in range(4):
            store(i, c).start()

    run("first", gate_parts, 0)
    run("first", [value_parts[p] for p in (1, 2, 0)], 0)
    gate_parts[0].second(0)
    out_parts[2].second(0)
    gate_parts[2].second(0)
    @pl.loop(0, 4)
    def _(c):
        @pl.loop(0, 16, init_carry=(none,) * 31)
        def tap_sums(b, carry):
            at = pl.multiple_of(b * 32, 32)
            grad = gext[c, pl.ds(at + 16, 32)]
            return tuple(
                carry[k] + fold(grad * ext[c, pl.ds(at + (k + 1), 32)]) for k in range(31)
            )

        for k in range(31):
            cols[c, k : k + 1] = jnp.sum(tap_sums[k], axis=0, keepdims=True)

    tiny.send(0)
    gate_parts[1].second(0)
    out_parts[0].third(0)
    out_parts[0].first(1)
    out_parts[1].third(0)
    run("second", [value_parts[p] for p in (2, 0)], 0)
    out_parts[1].first(1)
    value_parts[1].second(0)
    out_parts[2].third(0)
    tiny.collect(0)
    tiny.send(1)
    gate_parts[0].third(0)
    out_parts[2].first(1)
    gate_parts[0].first(1)
    gate_parts[2].third(0)
    gate_parts[2].first(1)
    out_parts[0].second(1)
    gate_parts[1].third(0)
    gate_parts[1].first(1)
    value_parts[0].third(0)
    value_parts[0].first(1)
    run("third", [value_parts[p] for p in (2, 1)], 0)
    value_parts[1].first(1)
    tiny.collect(1)
    tiny.send(2)
    value_parts[2].first(1)
    run("second", [out_parts[p] for p in (2, 1)], 1)
    gate_parts[0].second(1)
    out_parts[0].third(1)
    out_parts[0].first(2)
    run("second", [gate_parts[p] for p in (1, 2)], 1)
    run("second", value_parts, 1)
    gate_parts[0].third(1)
    gate_parts[0].first(2)
    out_parts[1].third(1)
    out_parts[1].first(2)
    out_parts[2].third(1)
    tiny.collect(2)
    tiny.send(3)
    out_parts[2].first(2)
    out_parts[0].second(2)
    gate_parts[1].third(1)
    gate_parts[1].first(2)
    value_parts[0].third(1)
    value_parts[0].first(2)
    value_parts[1].third(1)
    value_parts[1].first(2)
    gate_parts[2].third(1)
    gate_parts[2].first(2)
    value_parts[2].third(1)
    value_parts[2].first(2)
    out_parts[1].second(2)
    gate_parts[0].second(2)
    out_parts[0].third(2)
    out_parts[2].second(2)
    gate_parts[1].second(2)
    value_parts[0].second(2)
    gate_parts[2].second(2)
    run("second", [value_parts[p] for p in (1, 2)], 2)
    gate_parts[0].third(2)
    out_parts[1].third(2)
    out_parts[2].third(2)
    leave(2).start()
    gate_parts[1].third(2)
    gate_parts[2].third(2)
    leave(1).start()
    value_parts[0].third(2)
    value_parts[1].third(2)
    value_parts[2].third(2)
    leave(0).start()
    tiny.collect(3)
    leave(3).start()

    tiny.drain()
    for part in (*out_parts, *value_parts, *gate_parts):
        for stage in range(3):
            part.drain(stage)
    for k in range(4):
        give(feat_hbm, feat, f_ssem, f_rsem, k).wait_send()
        give(cot_hbm, cot, c_ssem, c_rsem, k).wait_send()
    for i in range(2):
        edge(edges, edges_in, i, 0).wait_send()
        edge(gedges, gedges_in, i, 2).wait_send()
        share(i).wait_send()
        for c in range(4):
            store(i, c).wait()
    for i in range(4):
        leave(i).wait()


def hand_kernel(vgrad, ggrad, vw, gw, ow, small, vgrad_o, ggrad_o, vw_o, gw_o, ow_o,
                taps_o, gain_o, big, mid, tiny, taps, gain, in_sem, out_sem):
    moves = []
    for i, (src, dst) in enumerate(((vgrad, vgrad_o), (ggrad, ggrad_o))):
        for q in range(4):
            rows = pl.ds(q * 128, 128)
            moves.append((src.at[rows], big.at[i, rows], [(big.at[i, rows], dst.at[rows])]))
    for i, (src, dst) in enumerate(((vw, vw_o), (gw, gw_o), (ow, ow_o))):
        moves.append((src, mid.at[i], [(mid.at[i], dst)]))
    moves.append((small, tiny, [(taps, taps_o), (gain, gain_o)]))
    ins = [
        pltpu.make_async_copy(src, held, in_sem.at[i]) for i, (src, held, _) in enumerate(moves)
    ]
    outs, at = [], 0
    for copy in ins:
        copy.start()
    for copy, (_, _, goes) in zip(ins, moves):
        copy.wait()
        if len(goes) == 2:
            taps[...] = tiny[0:31]
            gain[...] = tiny[31:32]
        for src, dst in goes:
            outs.append(pltpu.make_async_copy(src, dst, out_sem.at[at]))
            outs[-1].start()
            at += 1
    for copy in outs:
        copy.wait()


def on_device(features, weight_value, weight_gate, weight_out, conv_taps, norm_gain, out_grad):
    grad = jax.ShapeDtypeStruct((512, 512), F32)
    piece = jax.ShapeDtypeStruct((64, 512), F32)
    vmem = pl.BlockSpec(memory_space=pltpu.VMEM)
    hbm = pl.BlockSpec(memory_space=pl.ANY)
    dma = pltpu.SemaphoreType.DMA
    tiles = (4, 512, 128)
    vgrad, ggrad, vw, gw, ow, small = pl.pallas_call(
        whole_kernel,
        out_shape=(grad, grad, piece, piece, piece, jax.ShapeDtypeStruct((32, 512), F32)),
        in_specs=[hbm, hbm, hbm, hbm, vmem, vmem, hbm],
        out_specs=(hbm,) * 6,
        scratch_shapes=[
            *[pltpu.VMEM((64, 512), F32)] * 3,
            pltpu.VMEM((32, 512), F32),
            pltpu.VMEM((2, 512, 2048), BF16),
            pltpu.VMEM((2, 512, 2048), BF16),
            pltpu.VMEM((4, 4, 4, 64, 512), BF16),
            pltpu.VMEM((4, 4, 4, 64, 512), BF16),
            pltpu.VMEM((3, 2, 512, 512), BF16),
            pltpu.VMEM((3, 512, 512), BF16),
            pltpu.VMEM(tiles, F32),
            pltpu.VMEM(tiles, F32),
            pltpu.VMEM(tiles, F32),
            pltpu.VMEM(tiles, BF16),
            pltpu.VMEM(tiles, BF16),
            pltpu.VMEM((4, 544, 128), F32),
            pltpu.VMEM((4, 544, 128), F32),
            pltpu.VMEM((4, 32, 128), F32),
            pltpu.VMEM((4, 8, 128), F32),
            pltpu.VMEM((512, 512), BF16),
            pltpu.VMEM((512, 512), BF16),
            pltpu.VMEM((512, 512), BF16),
            pltpu.VMEM((2, 4, 16, 128), BF16),
            pltpu.VMEM((2, 4, 16, 128), BF16),
            pltpu.VMEM((2, 4, 16, 128), F32),
            pltpu.VMEM((2, 4, 16, 128), F32),
            pltpu.VMEM((2, 2, 512, 128), F32),
            pltpu.VMEM((2, 2, 512, 128), F32),
            pltpu.VMEM((512, 128), F32),
            pltpu.VMEM((4, 32, 128), F32),
            pltpu.VMEM((4, 4, 32, 128), F32),
            pltpu.VMEM((3, 32, 128), F32),
            dma((3, 2)), dma((3,)),
            dma((4,)), dma((4,)), dma((4,)),
            dma((4,)), dma((4,)), dma((4,)),
            dma((4,)), dma((4,)), dma((2,)), dma((2,)), dma((2, 4)), dma((4,)),
            dma((16,)), dma((16,)),
            *part_scratch(),
        ],
        compiler_params=pltpu.CompilerParams(
            collective_id=0, has_side_effects=True, vmem_limit_bytes=64 * 1024 * 1024 - 65536
        ),
    )(features, weight_value, weight_gate, weight_out, conv_taps, norm_gain[None], out_grad)
    *rest, gain = pl.pallas_call(
        hand_kernel,
        out_shape=(
            grad, grad, piece, piece, piece,
            jax.ShapeDtypeStruct((31, 512), F32), jax.ShapeDtypeStruct((1, 512), F32),
        ),
        in_specs=[hbm] * 6,
        out_specs=(hbm,) * 7,
        scratch_shapes=[
            pltpu.VMEM((2, 512, 512), F32),
            pltpu.VMEM((3, 64, 512), F32),
            pltpu.VMEM((32, 512), F32),
            pltpu.VMEM((31, 512), F32),
            pltpu.VMEM((1, 512), F32),
            dma((12,)), dma((13,)),
        ],
    )(vgrad, ggrad, vw, gw, ow, small)
    return (*rest, gain[0])


def solution(mesh):
    return jax.shard_map(
        on_device,
        mesh=mesh,
        in_specs=(
            P(SP, "tp"), P(None, "tp"), P(None, "tp"), P(None, "tp"),
            P(None, "tp"), P("tp"), P(SP, "tp"),
        ),
        out_specs=(
            P(SP, "tp"), P(SP, "tp"), P(SP, "tp"), P(SP, "tp"), P(SP, "tp"),
            P(None, "tp"), P("tp"),
        ),
        check_vma=False,
    )
```

```python
import functools

import jax
import jax.numpy as jnp
from jax import lax
from jax.experimental import pallas as pl
from jax.experimental.pallas import tpu as pltpu
from jax.sharding import PartitionSpec as P

SP = "sp"
MESH = pl.DeviceIdType.MESH
BF16 = jnp.bfloat16
F32 = jnp.float32

NORM_EPS = 1e-05

WIDTHS = ((128, 128, 256), (256, 128, 128), (128, 256, 128))
ORDERS = ("xzy", "yxz", "zyx")
ROWS = (512, 128, 32)
SENT = (BF16, BF16, BF16)


def coords():
    sp = lax.axis_index("sp")
    return {"z": sp // 16, "y": (sp // 4) % 4, "x": sp % 4}


def peer(where, dim, shift):
    to = dict(where)
    to[dim] = (where[dim] + shift + 4) % 4
    return (to["z"] * 16 + to["y"] * 4 + to["x"], lax.axis_index("tp"))


def remote(src, dst, ssem, rsem, device):
    return pltpu.make_async_remote_copy(
        src_ref=src, dst_ref=dst, send_sem=ssem, recv_sem=rsem,
        device_id=device, device_id_type=MESH,
    )


class Part:
    def __init__(self, where, p, lhs_t, rhs, cols, out, bufs, sems, spare):
        self.where, self.p, self.lhs_t, self.rhs = where, p, lhs_t, rhs
        self.cols, self.out, self.bufs, self.sems, self.spare = cols, out, bufs, sems, spare

    def source(self, stage, h, j):
        off, width = self.cols
        if stage == 0:
            if self.p == 0:
                rows = self.lhs_t[pl.ds(2 * h, 2), :, j]
            elif self.p == 1:
                rows = self.lhs_t[:, j, pl.ds(2 * h, 2)]
            else:
                rows = self.lhs_t[j, pl.ds(2 * h, 2)]
            rows = rows.reshape(512, rows.shape[-1])
            return jnp.dot(rows, self.rhs[:, off : off + width], preferred_element_type=F32)
        held = self.bufs[stage - 1][2]
        if stage == 1:
            if self.p == 1:
                at = (j // 2) * 8 + j % 2
                two = [held[at + 2 * (2 * h + i)] for i in range(2)]
                return jnp.concatenate(two, axis=0)
        return held[pl.ds(4 * j + 2 * h, 2)].reshape(128, width)

    def place(self, stage, h, value):
        width = self.cols[1]
        held = self.bufs[stage][2]
        count = ROWS[stage] // 64
        held[pl.ds(count * h, count)] = value.reshape(count, 64, width)

    def sender(self, stage, slot):
        send = self.bufs[stage][0]
        if send is not None:
            return send.at[slot]
        off, width = self.cols
        lanes = pl.ds(pl.multiple_of((slot % 3) * 512 + off, 128), width)
        return self.spare.at[slot // 3, :, lanes]

    def copy(self, stage, slot, sem, sign):
        recv = self.bufs[stage][1]
        ssem, rsem = self.sems
        return remote(
            recv.at[slot] if isinstance(slot, pl.Slice) else self.sender(stage, slot),
            recv.at[slot], ssem.at[stage], rsem.at[stage * 4 + sem],
            peer(self.where, ORDERS[self.p][stage], sign),
        )

    def straight(self, k):
        send, recv, _ = self.bufs[2]
        ssem, rsem = self.sems
        return remote(send.at[k], recv.at[k], ssem.at[2], rsem.at[8 + k],
                      peer(self.where, ORDERS[self.p][2], k + 1))

    def first(self, stage):
        m = self.where[ORDERS[self.p][stage]]
        if stage == 2:
            for k in (1, 0, 2):
                self.bufs[2][0][k] = self.bufs[1][2][(m + k + 1) % 4].astype(BF16)
            for k in (1, 0, 2):
                self.straight(k).start()
            return

        @pl.loop(0, 4)
        def _(i):
            sign = 1 - 2 * (i % 2)
            h = ((i + 1) // 2) % 2
            j = (m + 6 - (i // 2) * sign) % 4
            slot = i + (i // 2) * (2 - 3 * (i % 2))
            self.sender(stage, slot)[...] = self.source(stage, h, j).astype(SENT[stage])
            self.copy(stage, slot, i + (i // 2) * sign, sign).start()

    def second(self, stage):
        m = self.where[ORDERS[self.p][stage]]
        recv = self.bufs[stage][1]

        @pl.loop(0, 2)
        def _(k):
            sign = 1 - 2 * k
            self.copy(stage, k, k, sign).wait_recv()
            mine = self.source(stage, k, (m + 4 + sign) % 4)
            slot = 3 + 2 * k
            total = mine + recv[k].astype(F32)
            self.sender(stage, slot)[...] = total.astype(SENT[stage])
            self.copy(stage, slot, 2 + k, sign).start()

    def third(self, stage):
        m = self.where[ORDERS[self.p][stage]]
        recv = self.bufs[stage][1]
        if stage == 2:
            total = self.bufs[1][2][m]
            for k in range(3):
                self.straight(k).wait_recv()
                total = total + recv[k].astype(F32)
            off, width = self.cols
            self.out[:, off : off + width] = total
            return

        @pl.loop(0, 2)
        def _(h):
            mine = self.source(stage, h, m)
            self.copy(stage, pl.ds(2 + 2 * h, 2), 2 + h, 1).wait_recv()
            total = mine + recv[2 + 2 * h].astype(F32) + recv[3 + 2 * h].astype(F32)
            self.place(stage, h, total)

    def drain(self, stage):
        if stage == 2:
            recv = self.bufs[2][1]
            ssem, rsem = self.sems
            to = peer(self.where, ORDERS[self.p][2], 1)
            remote(recv, recv, ssem.at[2], rsem.at[8], to).wait_send()
            return
        self.copy(stage, pl.ds(0, 6), 0, 1).wait_send()


class Gathered(Part):
    def own_rows(self, h):
        m = self.where[ORDERS[self.p][0]]
        return ring_piece(self.lhs_t, self.p, m, h)[...].reshape(512, 512)

    def ring(self, src, dst, sem, sign):
        ssem, rsem = self.sems
        return remote(src, dst, ssem.at[0], rsem.at[sem],
                      peer(self.where, ORDERS[self.p][0], sign))

    def first(self, stage):
        if stage:
            return Part.first(self, stage)
        off, width = self.cols
        recv, mine = self.bufs[0][1], self.rhs.at[:, off : off + width]
        self.ring(mine, recv.at[0], 0, 1).start()
        self.ring(mine, recv.at[1], 1, -1).start()

    def second(self, stage):
        if stage:
            return Part.second(self, stage)
        recv = self.bufs[0][1]
        for k, sign in enumerate((1, -1)):
            self.ring(recv.at[k], recv.at[k], k, sign).wait_recv()
            rows = pl.ds(256 * k, 256)
            self.ring(recv.at[k, rows], recv.at[2, rows], 2, sign).start()

    def middle(self, stage):
        off, width = self.cols
        recv, held = self.bufs[0][1:]

        @pl.loop(0, 2)
        def _(h):
            got = jnp.dot(self.own_rows(h), self.rhs[:, off : off + width],
                          preferred_element_type=F32)
            for slot in range(2):
                rows = self.lhs[slot, h].reshape(512, 512)
                got = got + jnp.dot(rows, recv[slot], preferred_element_type=F32)
            held[pl.ds(8 * h, 8)] = got.reshape(8, 64, width)

    def third(self, stage):
        if stage:
            return Part.third(self, stage)
        width = self.cols[1]
        recv, held = self.bufs[0][1:]
        self.ring(recv.at[2], recv.at[2], 2, 1).wait_recv()

        @pl.loop(0, 2)
        def _(h):
            rows = self.lhs[2, h].reshape(512, 512)
            got = jnp.dot(rows, recv[2], preferred_element_type=F32)
            held[pl.ds(8 * h, 8)] += got.reshape(8, 64, width)

    def source(self, stage, h, j):
        if stage == 1 and self.p == 1:
            held = self.bufs[0][2]
            two = [held[(2 * h + i) * 4 + j] for i in range(2)]
            return jnp.concatenate(two, axis=0)
        return Part.source(self, stage, h, j)

    def drain(self, stage):
        if stage:
            return Part.drain(self, stage)
        recv = self.bufs[0][1]
        self.ring(recv, recv, 0, 1).wait_send()


def ring_piece(rows_t, p, j, h):
    if p == 0:
        return rows_t.at[pl.ds(2 * h, 2), :, j]
    if p == 1:
        return rows_t.at[pl.ds(2 * h, 2), j]
    return rows_t.at[j, pl.ds(2 * h, 2)]


class Early:
    def __init__(self, where, p, rows_t, lhs, relay, sems):
        self.where, self.p, self.rows_t = where, p, rows_t
        self.lhs, self.relay = lhs, relay
        self.rsem, self.ysem, self.dsem, self.ssem, self.d_ssem = sems
        self.m, self.tp = where[ORDERS[p][0]], lax.axis_index("tp")

    def go(self, src, dst, ssem, rsem, sign):
        return remote(src, dst, self.ssem.at[ssem], rsem,
                      peer(self.where, ORDERS[self.p][0], sign))

    def when(self, shift, act):
        if self.p < 2:
            act()
        else:
            pl.when((self.m + 4 + shift) % 4 // 2 == self.tp)(act)

    def far_copies(self):
        j = (self.m + 2) % 4
        for k, sign in enumerate((1, -1)):
            if self.p < 2:
                src = ring_piece(self.rows_t, self.p, j, self.tp).at[k]
            else:
                src = ring_piece(self.rows_t, self.p, j, k)
            yield self.go(src, self.relay.at[k], 0, self.ysem.at[k], sign)

    def far(self):
        self.when(2, lambda: [c.start() for c in self.far_copies()] and None)

    def near_copies(self, k, q):
        sign = 1 - 2 * k
        j = (self.m + 4 + sign) % 4
        if self.p < 2:
            src = ring_piece(self.rows_t, self.p, j, self.tp).at[q]
            dst = self.lhs.at[k, self.tp, q]
        else:
            src, dst = ring_piece(self.rows_t, self.p, j, q), self.lhs.at[k, q]
        return self.go(src, dst, 1 + k, self.rsem.at[k], sign)

    def near(self, q):
        for k in range(2):
            self.when(1 - 2 * k, lambda: self.near_copies(k, q).start())

    def relays(self, k):
        dst = self.lhs.at[2, self.tp, k] if self.p < 2 else self.lhs.at[2, k]
        return self.go(self.relay.at[k], dst, 3 + k, self.rsem.at[2], 1 - 2 * k)

    def pass_on(self):
        def act(k):
            sign = 1 - 2 * k
            self.go(self.relay.at[k], self.relay.at[k], 0, self.ysem.at[k], sign).wait_recv()
            self.relays(k).start()

        for k in range(2):
            self.when(1 - 2 * k, lambda: act(k))

    def held(self, slot, half):
        return self.lhs.at[slot, half] if self.p < 2 else self.lhs.at[slot]

    def across(self, slot, half):
        ref = self.held(slot, half)
        return remote(ref, ref, self.d_ssem.at[slot], self.dsem.at[slot], partner())

    def share(self, slot):
        def act():
            ref = self.held(slot, self.tp)
            self.go(ref, ref, 0, self.rsem.at[slot], 1).wait_recv()
            self.across(slot, self.tp).start()

        self.when(0, act)

    def have(self, slot):
        wait = lambda: self.across(slot, 1 - self.tp).wait_recv()
        if self.p < 2:
            wait()
        else:
            pl.when(self.m // 2 != self.tp)(wait)

    def drain(self):
        two = lambda ref, sem: self.go(ref, ref, sem, self.rsem.at[0], 1).wait_send()
        self.when(2, lambda: two(self.relay, 0))
        for k in range(2):
            piece = self.lhs.at[k, 0] if self.p < 2 else self.lhs.at[k]
            self.when(1 - 2 * k, lambda: two(piece, 1 + k))
            self.when(1 - 2 * k, lambda: two(self.relay.at[k], 3 + k))
        for slot in range(3):
            self.when(0, lambda: self.across(slot, self.tp).wait_send())


class Small:
    def __init__(self, where, cols, slots, sums, out, sems):
        self.where, self.cols, self.slots = where, cols, slots
        self.sums, self.out, self.sems = sums, out, sems

    def copy(self, stage, d):
        dim = "xyzx"[stage]
        mine = self.where[dim]
        ssem, rsem = self.sems
        src = self.cols.at[(mine + d) % 4] if stage == 0 else self.sums.at[stage - 1]
        at = stage * 4 + d
        return remote(src, self.slots.at[stage, mine], ssem.at[at], rsem.at[at],
                      peer(self.where, dim, d))

    def send(self, stage):
        mine = self.where["xyzx"[stage]]
        if stage == 0:
            self.slots[0, mine] = self.cols[mine]
        else:
            self.slots[stage, mine] = self.sums[stage - 1]

        @pl.loop(1, 4)
        def _(d):
            self.copy(stage, d).start()

    def collect(self, stage):
        @pl.loop(1, 4)
        def _(d):
            self.copy(stage, d).wait_recv()

        if stage < 3:
            a, b, c, d = [self.slots[stage, j] for j in range(4)]
            self.sums[stage] = (a + b) + (c + d)
        else:
            for j in range(4):
                self.out[:, 128 * j : 128 * j + 128] = self.slots[3, j]

    def drain(self):
        for stage in range(4):
            @pl.loop(1, 4)
            def _(d):
                self.copy(stage, d).wait_send()


def greet(where):
    barrier = pltpu.get_barrier_semaphore()
    for to in others(where):
        pl.semaphore_signal(barrier, inc=1, device_id=to, device_id_type=MESH)
    return barrier


def partner():
    return (lax.axis_index("sp"), 1 - lax.axis_index("tp"))


def along(shift):
    return ((lax.axis_index("sp") + 64 + shift) % 64, lax.axis_index("tp"))


def others(where):
    near = [peer(where, dim, shift) for dim in "zyx" for shift in (1, 2, 3)]
    return near + [along(-1), along(1), partner()]


def part_scratch():
    shapes = []
    for r, widths in enumerate(WIDTHS):
        for width in widths:
            for stage in range(3):
                if stage == 0:
                    shapes.append(pltpu.VMEM((3 if r else 6, 512, width), BF16))
                else:
                    shape = pltpu.VMEM((6, 128, width) if stage == 1 else (3, 64, width), BF16)
                    shapes.append(shape)
                    shapes.append(shape)
                if stage < 2:
                    shapes.append(pltpu.VMEM((ROWS[stage] // 32, 64, width), F32))
            shapes.append(pltpu.SemaphoreType.DMA((3,)))
            shapes.append(pltpu.SemaphoreType.DMA((12,)))
    return shapes


def take_parts(where, r, lhs_t, rhs, out, pool, spare=None, lhs=(None,) * 3):
    parts, off = [], 0
    for p, width in enumerate(WIDTHS[r]):
        bufs = []
        for stage in range(3):
            recv = next(pool)
            send = None if stage == 0 else next(pool)
            bufs.append((send, recv, next(pool) if stage < 2 else None))
        sems = (next(pool), next(pool))
        kind = Gathered if r else Part
        part = kind(where, p, lhs_t, rhs, (off, width), out, bufs, sems, spare)
        part.lhs = lhs[p]
        parts.append(part)
        off += width
    return parts


def early_scratch():
    dma = pltpu.SemaphoreType.DMA
    shapes = []
    for p in range(3):
        shapes.append(pltpu.VMEM((3, 2, 2, 4, 64, 512), BF16))
        shapes.append(pltpu.VMEM((2, 4, 64, 512) if p < 2 else (2, 2, 4, 64, 512), BF16))
        shapes += [dma((3,)), dma((2,)), dma((3,)), dma((5,)), dma((3,))]
    return shapes


def flip(src, dst, h, k):
    for q in range(2):
        at = pl.multiple_of(k * 512 + q * 256, 256)
        cols = src[h, :, pl.ds(at, 256)]
        dst[h * 2 + k // 2, (k % 2) * 2 + q] = cols.T.reshape(4, 64, 512)


def lane_sum(a):
    return jnp.sum(a, axis=-1, keepdims=True)


def fold(a):
    return jnp.sum(a.reshape(-1, 8, 128), axis=0)


def whole_kernel(
    feat_hbm, wv_hbm, wg_hbm, wo_hbm, taps_in, gain_in, cot_hbm,
    vgrad_hbm, ggrad_hbm, vw_hbm, gw_hbm, ow_hbm, small_hbm,
    value_out, gate_out, out_out, small_out, feat, cot, feat_t, cot_t, wbuf, wobuf, acc0, acc1, acc2, vhalf, ghalf,
    ext, gext, taps, gains, act, vlow, glow, edges, edges_in, gedges, gedges_in,
    stats, stats_in, inv_rows, cols, slots, sums,
    w_sem, wo_sem, f_sem, f_ssem, f_rsem, c_sem, c_ssem, c_rsem,
    e_ssem, e_rsem, s_ssem, s_rsem, o_sem, r_sem, small_ssem, small_rsem, *pool,
):
    where = coords()
    sp, tp = lax.axis_index("sp"), lax.axis_index("tp")
    pool = iter(pool)
    tiny = Small(where, cols, slots, sums, small_out, (small_ssem, small_rsem))
    early = []
    for p in range(3):
        lhs, relay = next(pool), next(pool)
        early.append(Early(where, p, feat_t, lhs, relay, [next(pool) for _ in range(5)]))
    lhs = [e.lhs for e in early]
    out_parts = take_parts(where, 0, cot_t, act, out_out, pool, cot)
    value_parts = take_parts(where, 1, feat_t, vlow, value_out, pool, None, lhs)
    gate_parts = take_parts(where, 2, feat_t, glow, gate_out, pool, None, lhs)

    def start_round(parts):
        @pl.loop(0, 4)
        def _(i):
            sign = 1 - 2 * (i % 2)
            h = ((i + 1) // 2) % 2
            slot = i + (i // 2) * (2 - 3 * (i % 2))
            for part in parts:
                m = where[ORDERS[part.p][0]]
                j = (m + 6 - (i // 2) * sign) % 4
                part.sender(0, slot)[...] = part.source(0, h, j).astype(BF16)
            for part in parts:
                part.copy(0, slot, i + (i // 2) * sign, sign).start()

    def run(name, parts, stage):
        for part in parts:
            getattr(part, name)(stage)

    def half_of(k):
        return (tp + k // 4) % 2

    def w_loads(k):
        row = pl.multiple_of(half_of(k) * 2048 + (k % 4) * 512, 512)
        slot = k % 3
        return [
            pltpu.make_async_copy(w.at[pl.ds(row, 512)], wbuf.at[slot, i], w_sem.at[slot, i])
            for i, w in enumerate((wv_hbm, wg_hbm))
        ]

    def wo_load(k):
        row = pl.multiple_of(half_of(k) * 2048 + (k % 4) * 512, 512)
        slot = k % 3
        return pltpu.make_async_copy(wo_hbm.at[pl.ds(row, 512)], wobuf.at[slot], wo_sem.at[slot])

    def cut(k):
        return pl.ds(pl.multiple_of(k * 512, 512), 512)

    def own(src, dst, sem, k):
        return pltpu.make_async_copy(src.at[:, cut(k)], dst.at[tp, :, cut(k)], sem.at[k])

    def give(src, dst, ssem, rsem, k):
        return remote(
            src.at[:, cut(k)], dst.at[tp, :, cut(k)], ssem.at[k], rsem.at[k], partner()
        )

    barrier = greet(where)
    for k in range(4):
        own(feat_hbm, feat, f_sem, k).start()
    for k in range(3):
        for c in w_loads(k):
            c.start()
    for k in range(4):
        own(cot_hbm, cot, c_sem, k).start()
    for k in range(3):
        wo_load(k).start()

    acc0[...] = jnp.zeros_like(acc0)
    acc1[...] = jnp.zeros_like(acc1)
    acc2[...] = jnp.zeros_like(acc2)
    for c in range(4):
        taps[c, 0:31] = taps_in[:, 128 * c : 128 * c + 128]
        gains[c] = jnp.broadcast_to(gain_in[:, 128 * c : 128 * c + 128], (8, 128))

    def add_dot(acc, x, w):
        for c in range(2):
            got = jnp.dot(x, w[:, 256 * c : 256 * c + 256], preferred_element_type=F32)
            acc[2 * c] += got[:, :128]
            acc[2 * c + 1] += got[:, 128:]

    def project(lo, hi, arrived):
        @pl.loop(lo, hi)
        def _(k):
            for c in w_loads(k):
                c.wait()
            arrived(k % 4)
            x = feat[half_of(k), :, cut(k % 4)]
            for i, acc in enumerate((acc0, acc1)):
                add_dot(acc, x, wbuf[k % 3, i])

            @pl.when(k + 3 < 8)
            def _():
                for c in w_loads(k + 3):
                    c.start()

    def cot_step(lo, hi, arrived):
        @pl.loop(lo, hi)
        def _(k):
            wo_load(k).wait()
            arrived(k % 4)
            h = half_of(k)
            add_dot(acc2, cot[h, :, cut(k % 4)], wobuf[k % 3])
            flip(cot, cot_t, h, k % 4)

            @pl.when(k + 3 < 8)
            def _():
                wo_load(k + 3).start()

    @pl.loop(0, 4)
    def _(k):
        own(feat_hbm, feat, f_sem, k).wait()
        flip(feat, feat_t, tp, k)

    pl.semaphore_wait(barrier, 12)
    for k in range(4):
        give(feat_hbm, feat, f_ssem, f_rsem, k).start()
    for e in early:
        e.far()
    for k in range(4):
        give(cot_hbm, cot, c_ssem, c_rsem, k).start()
    for q in range(2):
        for e in early[1:]:
            e.near(q)
    project(0, 4, lambda k: None)
    cot_step(0, 4, lambda k: own(cot_hbm, cot, c_sem, k).wait())
    project(4, 8, lambda k: give(feat_hbm, feat, f_ssem, f_rsem, k).wait_recv())

    def gate_rows(at):
        kept = []
        for c in range(4):
            value = acc0[c, pl.ds(at, 32)].astype(BF16)
            gate = acc1[c, pl.ds(at, 32)].astype(BF16)
            vhalf[c, pl.ds(at, 32)] = value
            ghalf[c, pl.ds(at, 32)] = gate
            sig = jax.nn.sigmoid(gate.astype(F32))
            mixed = (value.astype(F32) * sig).astype(BF16)
            ext[c, pl.ds(at + 16, 32)] = mixed.astype(F32)
            kept.append(mixed)
        return kept

    def edge(send, recv, i, at):
        return remote(send.at[i], recv.at[i], e_ssem.at[at + i], e_rsem.at[at + i],
                      along(2 * i - 1))

    for i, kept in enumerate((gate_rows(0), gate_rows(480))):
        for c in range(4):
            edges[i, c] = kept[c][16 * i : 16 * i + 16]
    for i in range(2):
        edge(edges, edges_in, i, 0).start()
    for q in range(2):
        early[0].near(q)

    @pl.loop(1, 15)
    def _(b):
        gate_rows(pl.multiple_of(b * 32, 32))

    cot_step(4, 8, lambda k: give(cot_hbm, cot, c_ssem, c_rsem, k).wait_recv())

    def fill(buf, got, i):
        inside = sp > 0 if i == 0 else sp < 63
        for c in range(4):
            rows = got[1 - i, c].astype(F32)
            buf[c, 528 * i : 528 * i + 16] = jnp.where(inside, rows, 0.0)

    def conv(buf, c, at, first, step):
        total = jnp.zeros((64, 128), F32)
        for k in range(31):
            rows = buf[c, pl.ds(at + (first + step * k), 64)]
            total = total + taps[c, k : k + 1] * rows
        return total

    def share(n):
        return remote(stats.at[n], stats_in.at[n], s_ssem.at[n], s_rsem.at[n], partner())

    def conv_rows(b):
        at = pl.multiple_of(b * 64, 64)
        zero = jnp.zeros((64, 128), F32)

        @pl.loop(0, 4, init_carry=(zero, zero))
        def totals(c, carry):
            got = conv(ext, c, at, 1, 1)
            acc0[c, pl.ds(at, 64)] = got
            return carry[0] + got, carry[1] + got * got

        stats[0, 0, pl.ds(at, 64)] = totals[0]
        stats[0, 1, pl.ds(at, 64)] = totals[1]

    pl.loop(1, 7)(conv_rows)
    for i in range(2):
        edge(edges, edges_in, 1 - i, 0).wait_recv()
        fill(ext, edges_in, i)

    pl.loop(0, 8, step=7)(conv_rows)
    share(0).start()

    @pl.loop(0, 4)
    def _(k):
        flip(feat, feat_t, 1 - tp, k)

    share(0).wait_recv()

    none = jnp.zeros((8, 128), F32)

    @pl.loop(0, 16, init_carry=(none,) * 4)
    def gain_sums(b, carry):
        at = pl.multiple_of(b * 32, 32)
        rows = pl.ds(at, 32)
        mean = lane_sum(stats[0, 0, rows] + stats_in[0, 0, rows]) / 1024
        square = lane_sum(stats[0, 1, rows] + stats_in[0, 1, rows]) / 1024
        inv = lax.rsqrt(square - mean * mean + NORM_EPS)
        inv_rows[rows] = jnp.broadcast_to(inv, (32, 128))
        first = jnp.zeros((32, 128), F32)
        second = jnp.zeros((32, 128), F32)
        carried = []
        for c in range(4):
            gain = gains[c, 0:1]
            normed = (acc0[c, rows] - mean) * inv
            pre = normed * gain
            sig = jax.nn.sigmoid(pre)
            act[rows, 128 * c : 128 * c + 128] = (pre * sig).astype(BF16)
            grad = acc2[c, rows] * sig * (1.0 + pre * (1.0 - sig))
            carried.append(carry[c] + fold(grad * normed))
            ngrad = grad * gain
            acc0[c, rows] = normed
            acc1[c, rows] = ngrad
            first = first + ngrad
            second = second + ngrad * normed
        stats[1, 0, rows] = first
        stats[1, 1, rows] = second
        return tuple(carried)

    share(1).start()
    for c in range(4):
        cols[c, 31:32] = jnp.sum(gain_sums[c], axis=0, keepdims=True)
    run("first", out_parts[2:], 0)
    share(1).wait_recv()

    def conv_grad(at):
        rows = pl.ds(at, 32)
        m1 = lane_sum(stats[1, 0, rows] + stats_in[1, 0, rows]) / 1024
        m2 = lane_sum(stats[1, 1, rows] + stats_in[1, 1, rows]) / 1024
        kept = []
        for c in range(4):
            got = inv_rows[rows] * (acc1[c, rows] - m1 - acc0[c, rows] * m2)
            gext[c, pl.ds(at + 16, 32)] = got
            kept.append(got)
        return kept

    for i, kept in enumerate((conv_grad(0), conv_grad(480))):
        for c in range(4):
            gedges[i, c] = kept[c][16 * i : 16 * i + 16]
    for i in range(2):
        edge(gedges, gedges_in, i, 2).start()

    start_round(out_parts[:2])

    @pl.loop(1, 15)
    def _(b):
        conv_grad(pl.multiple_of(b * 32, 32))

    def grad_rows(b):
        at = pl.multiple_of(b * 64, 64)
        rows = pl.ds(at, 64)

        @pl.loop(0, 4)
        def _(c):
            mixed_grad = conv(gext, c, at, 31, -1)
            value = vhalf[c, rows].astype(F32)
            sig = jax.nn.sigmoid(ghalf[c, rows].astype(F32))
            vgrad = mixed_grad * sig
            ggrad = mixed_grad * value * sig * (1.0 - sig)
            acc0[c, rows] = vgrad
            acc1[c, rows] = ggrad
            lanes = pl.ds(pl.multiple_of(c * 128, 128), 128)
            vlow[rows, lanes] = vgrad.astype(BF16)
            glow[rows, lanes] = ggrad.astype(BF16)

    for e in early:
        for slot in range(2):
            e.share(slot)
    pl.loop(1, 7)(grad_rows)
    for i in range(2):
        edge(gedges, gedges_in, 1 - i, 2).wait_recv()
        fill(gext, gedges_in, i)

    pl.loop(0, 8, step=7)(grad_rows)

    def store(i, c):
        src, dst = ((acc0, vgrad_hbm), (acc1, ggrad_hbm))[i]
        return pltpu.make_async_copy(
            src.at[c], dst.at[:, 128 * c : 128 * c + 128], o_sem.at[i, c]
        )

    def leave(i):
        src = (value_out, gate_out, out_out, small_out)[i]
        dst = (vw_hbm, gw_hbm, ow_hbm, small_hbm)[i]
        return pltpu.make_async_copy(src, dst, r_sem.at[i])

    for i in range(2):
        for c in range(4):
            store(i, c).start()

    run("first", value_parts, 0)
    run("first", gate_parts, 0)
    for e in early:
        e.pass_on()
    value_parts[1].second(0)
    @pl.loop(0, 4)
    def _(c):
        @pl.loop(0, 16, init_carry=(none,) * 31)
        def tap_sums(b, carry):
            at = pl.multiple_of(b * 32, 32)
            grad = gext[c, pl.ds(at + 16, 32)]
            return tuple(
                carry[k] + fold(grad * ext[c, pl.ds(at + (k + 1), 32)]) for k in range(31)
            )

        for k in range(31):
            cols[c, k : k + 1] = jnp.sum(tap_sums[k], axis=0, keepdims=True)

    tiny.send(0)

    run("second", [out_parts[p] for p in (2, 0, 1)], 0)
    early[1].have(0)
    early[1].have(1)
    value_parts[1].middle(0)
    run("second", [value_parts[p] for p in (0, 2)], 0)
    early[0].have(0)
    early[0].have(1)
    early[2].have(0)
    early[2].have(1)
    run("middle", [value_parts[p] for p in (0, 2)], 0)
    run("second", [gate_parts[p] for p in (0, 1)], 0)
    gate_parts[0].middle(0)
    gate_parts[2].second(0)
    run("middle", [gate_parts[p] for p in (2, 1)], 0)
    early[0].share(2)
    early[1].share(2)
    run("third", [out_parts[p] for p in (0, 1)], 0)
    out_parts[1].first(1)
    tiny.collect(0)
    tiny.send(1)
    out_parts[0].first(1)
    early[1].have(2)
    early[0].have(2)
    run("third", [value_parts[p] for p in (1, 0)], 0)
    early[2].share(2)
    run("first", [value_parts[p] for p in (0, 1)], 1)
    gate_parts[0].third(0)
    out_parts[2].third(0)
    out_parts[2].first(1)
    gate_parts[1].third(0)
    gate_parts[0].first(1)
    early[2].have(2)
    value_parts[2].third(0)
    gate_parts[1].first(1)
    value_parts[2].first(1)
    gate_parts[2].third(0)
    out_parts[1].second(1)
    value_parts[1].second(1)
    gate_parts[2].first(1)
    run("second", [out_parts[p] for p in (0, 2)], 1)
    tiny.collect(1)
    tiny.send(2)
    value_parts[0].second(1)
    gate_parts[1].second(1)
    value_parts[2].second(1)
    gate_parts[0].second(1)
    out_parts[1].third(1)
    out_parts[1].first(2)
    gate_parts[2].second(1)
    out_parts[0].third(1)
    out_parts[0].first(2)
    value_parts[1].third(1)
    value_parts[1].first(2)
    value_parts[0].third(1)
    out_parts[2].third(1)
    tiny.collect(2)
    tiny.send(3)
    out_parts[2].first(2)
    value_parts[0].first(2)
    gate_parts[1].third(1)
    gate_parts[1].first(2)
    gate_parts[0].third(1)
    gate_parts[0].first(2)
    value_parts[2].third(1)
    value_parts[2].first(2)
    gate_parts[2].third(1)
    gate_parts[2].first(2)
    out_parts[1].third(2)
    out_parts[0].third(2)
    value_parts[1].third(2)
    value_parts[0].third(2)
    out_parts[2].third(2)
    leave(2).start()
    value_parts[2].third(2)
    leave(0).start()
    gate_parts[1].third(2)
    gate_parts[0].third(2)
    gate_parts[2].third(2)
    leave(1).start()
    tiny.collect(3)
    leave(3).start()

    tiny.drain()
    for e in early:
        e.drain()
    for part in (*out_parts, *value_parts, *gate_parts):
        for stage in range(3):
            part.drain(stage)
    for k in range(4):
        give(feat_hbm, feat, f_ssem, f_rsem, k).wait_send()
        give(cot_hbm, cot, c_ssem, c_rsem, k).wait_send()
    for i in range(2):
        edge(edges, edges_in, i, 0).wait_send()
        edge(gedges, gedges_in, i, 2).wait_send()
        share(i).wait_send()
        for c in range(4):
            store(i, c).wait()
    for i in range(4):
        leave(i).wait()


def hand_kernel(vgrad, ggrad, vw, gw, ow, small, vgrad_o, ggrad_o, vw_o, gw_o, ow_o,
                taps_o, gain_o, big, mid, tiny, taps, gain, in_sem, out_sem):
    moves = []
    for i, (src, dst) in enumerate(((vgrad, vgrad_o), (ggrad, ggrad_o))):
        for q in range(4):
            rows = pl.ds(q * 128, 128)
            moves.append((src.at[rows], big.at[i, rows], [(big.at[i, rows], dst.at[rows])]))
    for i, (src, dst) in enumerate(((vw, vw_o), (gw, gw_o), (ow, ow_o))):
        moves.append((src, mid.at[i], [(mid.at[i], dst)]))
    moves.append((small, tiny, [(taps, taps_o), (gain, gain_o)]))
    ins = [
        pltpu.make_async_copy(src, held, in_sem.at[i]) for i, (src, held, _) in enumerate(moves)
    ]
    outs, at = [], 0
    for copy in ins:
        copy.start()
    for copy, (_, _, goes) in zip(ins, moves):
        copy.wait()
        if len(goes) == 2:
            taps[...] = tiny[0:31]
            gain[...] = tiny[31:32]
        for src, dst in goes:
            outs.append(pltpu.make_async_copy(src, dst, out_sem.at[at]))
            outs[-1].start()
            at += 1
    for copy in outs:
        copy.wait()


def on_device(features, weight_value, weight_gate, weight_out, conv_taps, norm_gain, out_grad):
    grad = jax.ShapeDtypeStruct((512, 512), F32)
    piece = jax.ShapeDtypeStruct((64, 512), F32)
    vmem = pl.BlockSpec(memory_space=pltpu.VMEM)
    hbm = pl.BlockSpec(memory_space=pl.ANY)
    dma = pltpu.SemaphoreType.DMA
    tiles = (4, 512, 128)
    vgrad, ggrad, vw, gw, ow, small = pl.pallas_call(
        whole_kernel,
        out_shape=(grad, grad, piece, piece, piece, jax.ShapeDtypeStruct((32, 512), F32)),
        in_specs=[hbm, hbm, hbm, hbm, vmem, vmem, hbm],
        out_specs=(hbm,) * 6,
        scratch_shapes=[
            *[pltpu.VMEM((64, 512), F32)] * 3,
            pltpu.VMEM((32, 512), F32),
            pltpu.VMEM((2, 512, 2048), BF16),
            pltpu.VMEM((2, 512, 2048), BF16),
            pltpu.VMEM((4, 4, 4, 64, 512), BF16),
            pltpu.VMEM((4, 4, 4, 64, 512), BF16),
            pltpu.VMEM((3, 2, 512, 512), BF16),
            pltpu.VMEM((3, 512, 512), BF16),
            pltpu.VMEM(tiles, F32),
            pltpu.VMEM(tiles, F32),
            pltpu.VMEM(tiles, F32),
            pltpu.VMEM(tiles, BF16),
            pltpu.VMEM(tiles, BF16),
            pltpu.VMEM((4, 544, 128), F32),
            pltpu.VMEM((4, 544, 128), F32),
            pltpu.VMEM((4, 32, 128), F32),
            pltpu.VMEM((4, 8, 128), F32),
            pltpu.VMEM((512, 512), BF16),
            pltpu.VMEM((512, 512), BF16),
            pltpu.VMEM((512, 512), BF16),
            pltpu.VMEM((2, 4, 16, 128), BF16),
            pltpu.VMEM((2, 4, 16, 128), BF16),
            pltpu.VMEM((2, 4, 16, 128), F32),
            pltpu.VMEM((2, 4, 16, 128), F32),
            pltpu.VMEM((2, 2, 512, 128), F32),
            pltpu.VMEM((2, 2, 512, 128), F32),
            pltpu.VMEM((512, 128), F32),
            pltpu.VMEM((4, 32, 128), F32),
            pltpu.VMEM((4, 4, 32, 128), F32),
            pltpu.VMEM((3, 32, 128), F32),
            dma((3, 2)), dma((3,)),
            dma((4,)), dma((4,)), dma((4,)),
            dma((4,)), dma((4,)), dma((4,)),
            dma((4,)), dma((4,)), dma((2,)), dma((2,)), dma((2, 4)), dma((4,)),
            dma((16,)), dma((16,)),
            *early_scratch(),
            *part_scratch(),
        ],
        compiler_params=pltpu.CompilerParams(
            collective_id=0, has_side_effects=True, vmem_limit_bytes=64 * 1024 * 1024 - 65536
        ),
    )(features, weight_value, weight_gate, weight_out, conv_taps, norm_gain[None], out_grad)
    *rest, gain = pl.pallas_call(
        hand_kernel,
        out_shape=(
            grad, grad, piece, piece, piece,
            jax.ShapeDtypeStruct((31, 512), F32), jax.ShapeDtypeStruct((1, 512), F32),
        ),
        in_specs=[hbm] * 6,
        out_specs=(hbm,) * 7,
        scratch_shapes=[
            pltpu.VMEM((2, 512, 512), F32),
            pltpu.VMEM((3, 64, 512), F32),
            pltpu.VMEM((32, 512), F32),
            pltpu.VMEM((31, 512), F32),
            pltpu.VMEM((1, 512), F32),
            dma((12,)), dma((13,)),
        ],
    )(vgrad, ggrad, vw, gw, ow, small)
    return (*rest, gain[0])


def solution(mesh):
    return jax.shard_map(
        on_device,
        mesh=mesh,
        in_specs=(
            P(SP, "tp"), P(None, "tp"), P(None, "tp"), P(None, "tp"),
            P(None, "tp"), P("tp"), P(SP, "tp"),
        ),
        out_specs=(
            P(SP, "tp"), P(SP, "tp"), P(SP, "tp"), P(SP, "tp"), P(SP, "tp"),
            P(None, "tp"), P("tp"),
        ),
        check_vma=False,
    )
```

```python
import functools

import jax
import jax.numpy as jnp
from jax import lax
from jax.experimental import pallas as pl
from jax.experimental.pallas import tpu as pltpu
from jax.sharding import PartitionSpec as P

SP = "sp"
MESH = pl.DeviceIdType.MESH
BF16 = jnp.bfloat16
F32 = jnp.float32

NORM_EPS = 1e-05

WIDTHS = ((128, 256, 128), (128, 128, 256), (256, 128, 128))
ORDERS = ("xzy", "yxz", "zyx")
ROWS = (512, 128, 32)
SENT = (BF16, BF16, BF16)


def coords():
    sp = lax.axis_index("sp")
    return {"z": sp // 16, "y": (sp // 4) % 4, "x": sp % 4}


def peer(where, dim, shift):
    to = dict(where)
    to[dim] = (where[dim] + shift + 4) % 4
    return (to["z"] * 16 + to["y"] * 4 + to["x"], lax.axis_index("tp"))


def remote(src, dst, ssem, rsem, device):
    return pltpu.make_async_remote_copy(
        src_ref=src, dst_ref=dst, send_sem=ssem, recv_sem=rsem,
        device_id=device, device_id_type=MESH,
    )


class Part:
    def __init__(self, where, p, lhs_t, rhs, cols, out, bufs, sems, spare):
        self.where, self.p, self.lhs_t, self.rhs = where, p, lhs_t, rhs
        self.cols, self.out, self.bufs, self.sems, self.spare = cols, out, bufs, sems, spare

    def source(self, stage, h, j):
        off, width = self.cols
        if stage == 0:
            if self.p == 0:
                rows = self.lhs_t[pl.ds(2 * h, 2), :, j]
            elif self.p == 1:
                rows = self.lhs_t[:, j, pl.ds(2 * h, 2)]
            else:
                rows = self.lhs_t[j, pl.ds(2 * h, 2)]
            rows = rows.reshape(512, rows.shape[-1])
            return jnp.dot(rows, self.rhs[:, off : off + width], preferred_element_type=F32)
        held = self.bufs[stage - 1][2]
        if stage == 1:
            if self.p == 1:
                at = (j // 2) * 8 + j % 2
                two = [held[at + 2 * (2 * h + i)] for i in range(2)]
                return jnp.concatenate(two, axis=0)
        return held[pl.ds(4 * j + 2 * h, 2)].reshape(128, width)

    def place(self, stage, h, value):
        width = self.cols[1]
        held = self.bufs[stage][2]
        count = ROWS[stage] // 64
        held[pl.ds(count * h, count)] = value.reshape(count, 64, width)

    def sender(self, stage, slot):
        send = self.bufs[stage][0]
        if send is not None:
            return send.at[slot]
        off, width = self.cols
        lanes = pl.ds(pl.multiple_of((slot % 3) * 512 + off, 128), width)
        return self.spare.at[slot // 3, :, lanes]

    def copy(self, stage, slot, sem, sign):
        recv = self.bufs[stage][1]
        ssem, rsem = self.sems
        return remote(
            recv.at[slot] if isinstance(slot, pl.Slice) else self.sender(stage, slot),
            recv.at[slot], ssem.at[stage], rsem.at[stage * 4 + sem],
            peer(self.where, ORDERS[self.p][stage], sign),
        )

    def straight(self, k):
        send, recv, _ = self.bufs[2]
        ssem, rsem = self.sems
        return remote(send.at[k], recv.at[k], ssem.at[2], rsem.at[8 + k],
                      peer(self.where, ORDERS[self.p][2], k + 1))

    def first(self, stage):
        m = self.where[ORDERS[self.p][stage]]
        if stage == 2:
            for k in (1, 0, 2):
                self.bufs[2][0][k] = self.bufs[1][2][(m + k + 1) % 4].astype(BF16)
            for k in (1, 0, 2):
                self.straight(k).start()
            return

        @pl.loop(0, 4)
        def _(i):
            sign = 1 - 2 * (i % 2)
            h = ((i + 1) // 2) % 2
            j = (m + 6 - (i // 2) * sign) % 4
            slot = i + (i // 2) * (2 - 3 * (i % 2))
            self.sender(stage, slot)[...] = self.source(stage, h, j).astype(SENT[stage])
            self.copy(stage, slot, i + (i // 2) * sign, sign).start()

    def second(self, stage):
        m = self.where[ORDERS[self.p][stage]]
        recv = self.bufs[stage][1]

        @pl.loop(0, 2)
        def _(k):
            sign = 1 - 2 * k
            self.copy(stage, k, k, sign).wait_recv()
            mine = self.source(stage, k, (m + 4 + sign) % 4)
            slot = 3 + 2 * k
            total = mine + recv[k].astype(F32)
            self.sender(stage, slot)[...] = total.astype(SENT[stage])
            self.copy(stage, slot, 2 + k, sign).start()

    def third(self, stage):
        m = self.where[ORDERS[self.p][stage]]
        recv = self.bufs[stage][1]
        if stage == 2:
            total = self.bufs[1][2][m]
            for k in range(3):
                self.straight(k).wait_recv()
                total = total + recv[k].astype(F32)
            off, width = self.cols
            self.out[:, off : off + width] = total
            return

        @pl.loop(0, 2)
        def _(h):
            mine = self.source(stage, h, m)
            self.copy(stage, pl.ds(2 + 2 * h, 2), 2 + h, 1).wait_recv()
            total = mine + recv[2 + 2 * h].astype(F32) + recv[3 + 2 * h].astype(F32)
            self.place(stage, h, total)

    def drain(self, stage):
        if stage == 2:
            recv = self.bufs[2][1]
            ssem, rsem = self.sems
            to = peer(self.where, ORDERS[self.p][2], 1)
            remote(recv, recv, ssem.at[2], rsem.at[8], to).wait_send()
            return
        self.copy(stage, pl.ds(0, 6), 0, 1).wait_send()


class Gathered(Part):
    def own_rows(self, h):
        m = self.where[ORDERS[self.p][0]]
        return ring_piece(self.lhs_t, self.p, m, h)[...].reshape(512, 512)

    def ring(self, src, dst, sem, sign):
        ssem, rsem = self.sems
        return remote(src, dst, ssem.at[0], rsem.at[sem],
                      peer(self.where, ORDERS[self.p][0], sign))

    def first(self, stage):
        if stage:
            return Part.first(self, stage)
        off, width = self.cols
        recv, mine = self.bufs[0][1], self.rhs.at[:, off : off + width]
        self.ring(mine, recv.at[0], 0, 1).start()
        self.ring(mine, recv.at[1], 1, -1).start()

    def second(self, stage):
        if stage:
            return Part.second(self, stage)
        recv = self.bufs[0][1]
        for k, sign in enumerate((1, -1)):
            self.ring(recv.at[k], recv.at[k], k, sign).wait_recv()
            rows = pl.ds(256 * k, 256)
            self.ring(recv.at[k, rows], recv.at[2, rows], 2, sign).start()

    def middle(self, stage):
        off, width = self.cols
        recv, held = self.bufs[0][1:]

        @pl.loop(0, 2)
        def _(h):
            got = jnp.dot(self.own_rows(h), self.rhs[:, off : off + width],
                          preferred_element_type=F32)
            for slot in range(2):
                rows = self.lhs[slot, h].reshape(512, 512)
                got = got + jnp.dot(rows, recv[slot], preferred_element_type=F32)
            held[pl.ds(8 * h, 8)] = got.reshape(8, 64, width)

    def third(self, stage):
        if stage:
            return Part.third(self, stage)
        width = self.cols[1]
        recv, held = self.bufs[0][1:]
        self.ring(recv.at[2], recv.at[2], 2, 1).wait_recv()

        @pl.loop(0, 2)
        def _(h):
            rows = self.lhs[2, h].reshape(512, 512)
            got = jnp.dot(rows, recv[2], preferred_element_type=F32)
            held[pl.ds(8 * h, 8)] += got.reshape(8, 64, width)

    def source(self, stage, h, j):
        if stage == 1 and self.p == 1:
            held = self.bufs[0][2]
            two = [held[(2 * h + i) * 4 + j] for i in range(2)]
            return jnp.concatenate(two, axis=0)
        return Part.source(self, stage, h, j)

    def drain(self, stage):
        if stage:
            return Part.drain(self, stage)
        recv = self.bufs[0][1]
        self.ring(recv, recv, 0, 1).wait_send()


def ring_piece(rows_t, p, j, h):
    if p == 0:
        return rows_t.at[pl.ds(2 * h, 2), :, j]
    if p == 1:
        return rows_t.at[pl.ds(2 * h, 2), j]
    return rows_t.at[j, pl.ds(2 * h, 2)]


class Early:
    def __init__(self, where, p, rows_t, lhs, relay, sems):
        self.where, self.p, self.rows_t = where, p, rows_t
        self.lhs, self.relay = lhs, relay
        self.rsem, self.ysem, self.dsem, self.ssem, self.d_ssem = sems
        self.m, self.tp = where[ORDERS[p][0]], lax.axis_index("tp")

    def go(self, src, dst, ssem, rsem, sign):
        return remote(src, dst, self.ssem.at[ssem], rsem,
                      peer(self.where, ORDERS[self.p][0], sign))

    def when(self, shift, act):
        if self.p < 2:
            act()
        else:
            pl.when((self.m + 4 + shift) % 4 // 2 == self.tp)(act)

    def far_copies(self):
        j = (self.m + 2) % 4
        for k, sign in enumerate((1, -1)):
            if self.p < 2:
                src = ring_piece(self.rows_t, self.p, j, self.tp).at[k]
            else:
                src = ring_piece(self.rows_t, self.p, j, k)
            yield self.go(src, self.relay.at[k], 0, self.ysem.at[k], sign)

    def far(self):
        self.when(2, lambda: [c.start() for c in self.far_copies()] and None)

    def near_copies(self, k, q):
        sign = 1 - 2 * k
        j = (self.m + 4 + sign) % 4
        if self.p < 2:
            src = ring_piece(self.rows_t, self.p, j, self.tp).at[q]
            dst = self.lhs.at[k, self.tp, q]
        else:
            src, dst = ring_piece(self.rows_t, self.p, j, q), self.lhs.at[k, q]
        return self.go(src, dst, 1 + k, self.rsem.at[k], sign)

    def near(self, q):
        for k in range(2):
            self.when(1 - 2 * k, lambda: self.near_copies(k, q).start())

    def relays(self, k):
        dst = self.lhs.at[2, self.tp, k] if self.p < 2 else self.lhs.at[2, k]
        return self.go(self.relay.at[k], dst, 3 + k, self.rsem.at[2], 1 - 2 * k)

    def pass_on(self):
        def act(k):
            sign = 1 - 2 * k
            self.go(self.relay.at[k], self.relay.at[k], 0, self.ysem.at[k], sign).wait_recv()
            self.relays(k).start()

        for k in range(2):
            self.when(1 - 2 * k, lambda: act(k))

    def held(self, slot, half):
        return self.lhs.at[slot, half] if self.p < 2 else self.lhs.at[slot]

    def across(self, slot, half):
        ref = self.held(slot, half)
        return remote(ref, ref, self.d_ssem.at[slot], self.dsem.at[slot], partner())

    def share(self, slot):
        def act():
            ref = self.held(slot, self.tp)
            self.go(ref, ref, 0, self.rsem.at[slot], 1).wait_recv()
            self.across(slot, self.tp).start()

        self.when(0, act)

    def have(self, slot):
        wait = lambda: self.across(slot, 1 - self.tp).wait_recv()
        if self.p < 2:
            wait()
        else:
            pl.when(self.m // 2 != self.tp)(wait)

    def drain(self):
        two = lambda ref, sem: self.go(ref, ref, sem, self.rsem.at[0], 1).wait_send()
        self.when(2, lambda: two(self.relay, 0))
        for k in range(2):
            piece = self.lhs.at[k, 0] if self.p < 2 else self.lhs.at[k]
            self.when(1 - 2 * k, lambda: two(piece, 1 + k))
            self.when(1 - 2 * k, lambda: two(self.relay.at[k], 3 + k))
        for slot in range(3):
            self.when(0, lambda: self.across(slot, self.tp).wait_send())


class Small:
    def __init__(self, where, cols, slots, sums, out, sems):
        self.where, self.cols, self.slots = where, cols, slots
        self.sums, self.out, self.sems = sums, out, sems

    def copy(self, stage, d):
        dim = "xyzx"[stage]
        mine = self.where[dim]
        ssem, rsem = self.sems
        src = self.cols.at[(mine + d) % 4] if stage == 0 else self.sums.at[stage - 1]
        at = stage * 4 + d
        return remote(src, self.slots.at[stage, mine], ssem.at[at], rsem.at[at],
                      peer(self.where, dim, d))

    def send(self, stage):
        mine = self.where["xyzx"[stage]]
        if stage == 0:
            self.slots[0, mine] = self.cols[mine]
        else:
            self.slots[stage, mine] = self.sums[stage - 1]

        @pl.loop(1, 4)
        def _(d):
            self.copy(stage, d).start()

    def collect(self, stage):
        @pl.loop(1, 4)
        def _(d):
            self.copy(stage, d).wait_recv()

        if stage < 3:
            a, b, c, d = [self.slots[stage, j] for j in range(4)]
            self.sums[stage] = (a + b) + (c + d)
        else:
            for j in range(4):
                self.out[:, 128 * j : 128 * j + 128] = self.slots[3, j]

    def drain(self):
        for stage in range(4):
            @pl.loop(1, 4)
            def _(d):
                self.copy(stage, d).wait_send()


def greet(where):
    barrier = pltpu.get_barrier_semaphore()
    for to in others(where):
        pl.semaphore_signal(barrier, inc=1, device_id=to, device_id_type=MESH)
    return barrier


def partner():
    return (lax.axis_index("sp"), 1 - lax.axis_index("tp"))


def along(shift):
    return ((lax.axis_index("sp") + 64 + shift) % 64, lax.axis_index("tp"))


def others(where):
    near = [peer(where, dim, shift) for dim in "zyx" for shift in (1, 2, 3)]
    return near + [along(-1), along(1), partner()]


def part_scratch():
    shapes = []
    for r, widths in enumerate(WIDTHS):
        for width in widths:
            for stage in range(3):
                if stage == 0:
                    shapes.append(pltpu.VMEM((3 if r else 6, 512, width), BF16))
                else:
                    shape = pltpu.VMEM((6, 128, width) if stage == 1 else (3, 64, width), BF16)
                    shapes.append(shape)
                    shapes.append(shape)
                if stage < 2:
                    shapes.append(pltpu.VMEM((ROWS[stage] // 32, 64, width), F32))
            shapes.append(pltpu.SemaphoreType.DMA((3,)))
            shapes.append(pltpu.SemaphoreType.DMA((12,)))
    return shapes


def take_parts(where, r, lhs_t, rhs, out, pool, spare=None, lhs=(None,) * 3):
    parts, off = [], 0
    for p, width in enumerate(WIDTHS[r]):
        bufs = []
        for stage in range(3):
            recv = next(pool)
            send = None if stage == 0 else next(pool)
            bufs.append((send, recv, next(pool) if stage < 2 else None))
        sems = (next(pool), next(pool))
        kind = Gathered if r else Part
        part = kind(where, p, lhs_t, rhs, (off, width), out, bufs, sems, spare)
        part.lhs = lhs[p]
        parts.append(part)
        off += width
    return parts


def early_scratch():
    dma = pltpu.SemaphoreType.DMA
    shapes = []
    for p in range(3):
        shapes.append(pltpu.VMEM((3, 2, 2, 4, 64, 512), BF16))
        shapes.append(pltpu.VMEM((2, 4, 64, 512) if p < 2 else (2, 2, 4, 64, 512), BF16))
        shapes += [dma((3,)), dma((2,)), dma((3,)), dma((5,)), dma((3,))]
    return shapes


def flip(src, dst, h, k):
    for q in range(2):
        at = pl.multiple_of(k * 512 + q * 256, 256)
        cols = src[h, :, pl.ds(at, 256)]
        dst[h * 2 + k // 2, (k % 2) * 2 + q] = cols.T.reshape(4, 64, 512)


def lane_sum(a):
    return jnp.sum(a, axis=-1, keepdims=True)


def fold(a):
    return jnp.sum(a.reshape(-1, 8, 128), axis=0)


def whole_kernel(
    feat_hbm, wv_hbm, wg_hbm, wo_hbm, taps_in, gain_in, cot_hbm,
    vgrad_hbm, ggrad_hbm, vw_hbm, gw_hbm, ow_hbm, small_hbm,
    value_out, gate_out, out_out, small_out, feat, cot, feat_t, cot_t, wbuf, wobuf, acc0, acc1, acc2, vhalf, ghalf,
    ext, gext, taps, gains, act, vlow, glow, edges, edges_in, gedges, gedges_in,
    stats, stats_in, inv_rows, cols, slots, sums,
    w_sem, wo_sem, f_sem, f_ssem, f_rsem, c_sem, c_ssem, c_rsem,
    e_ssem, e_rsem, s_ssem, s_rsem, o_sem, r_sem, small_ssem, small_rsem, *pool,
):
    where = coords()
    sp, tp = lax.axis_index("sp"), lax.axis_index("tp")
    pool = iter(pool)
    tiny = Small(where, cols, slots, sums, small_out, (small_ssem, small_rsem))
    early = []
    for p in range(3):
        lhs, relay = next(pool), next(pool)
        early.append(Early(where, p, feat_t, lhs, relay, [next(pool) for _ in range(5)]))
    lhs = [e.lhs for e in early]
    out_parts = take_parts(where, 0, cot_t, act, out_out, pool, cot)
    value_parts = take_parts(where, 1, feat_t, vlow, value_out, pool, None, lhs)
    gate_parts = take_parts(where, 2, feat_t, glow, gate_out, pool, None, lhs)

    def start_round(parts):
        @pl.loop(0, 4)
        def _(i):
            sign = 1 - 2 * (i % 2)
            h = ((i + 1) // 2) % 2
            slot = i + (i // 2) * (2 - 3 * (i % 2))
            for part in parts:
                m = where[ORDERS[part.p][0]]
                j = (m + 6 - (i // 2) * sign) % 4
                part.sender(0, slot)[...] = part.source(0, h, j).astype(BF16)
            for part in parts:
                part.copy(0, slot, i + (i // 2) * sign, sign).start()

    def run(name, parts, stage):
        for part in parts:
            getattr(part, name)(stage)

    def half_of(k):
        return (tp + k // 4) % 2

    def w_loads(k):
        row = pl.multiple_of(half_of(k) * 2048 + (k % 4) * 512, 512)
        slot = k % 3
        return [
            pltpu.make_async_copy(w.at[pl.ds(row, 512)], wbuf.at[slot, i], w_sem.at[slot, i])
            for i, w in enumerate((wv_hbm, wg_hbm))
        ]

    def wo_load(k):
        row = pl.multiple_of(half_of(k) * 2048 + (k % 4) * 512, 512)
        slot = k % 3
        return pltpu.make_async_copy(wo_hbm.at[pl.ds(row, 512)], wobuf.at[slot], wo_sem.at[slot])

    def cut(k):
        return pl.ds(pl.multiple_of(k * 512, 512), 512)

    def own(src, dst, sem, k):
        return pltpu.make_async_copy(src.at[:, cut(k)], dst.at[tp, :, cut(k)], sem.at[k])

    def give(src, dst, ssem, rsem, k):
        return remote(
            src.at[:, cut(k)], dst.at[tp, :, cut(k)], ssem.at[k], rsem.at[k], partner()
        )

    barrier = greet(where)
    for k in range(4):
        own(feat_hbm, feat, f_sem, k).start()
    for k in range(3):
        for c in w_loads(k):
            c.start()
    for k in range(4):
        own(cot_hbm, cot, c_sem, k).start()
    for k in range(3):
        wo_load(k).start()

    acc0[...] = jnp.zeros_like(acc0)
    acc1[...] = jnp.zeros_like(acc1)
    acc2[...] = jnp.zeros_like(acc2)
    for c in range(4):
        taps[c, 0:31] = taps_in[:, 128 * c : 128 * c + 128]
        gains[c] = jnp.broadcast_to(gain_in[:, 128 * c : 128 * c + 128], (8, 128))

    def add_dot(acc, x, w):
        for c in range(2):
            got = jnp.dot(x, w[:, 256 * c : 256 * c + 256], preferred_element_type=F32)
            acc[2 * c] += got[:, :128]
            acc[2 * c + 1] += got[:, 128:]

    def project(lo, hi, arrived):
        @pl.loop(lo, hi)
        def _(k):
            for c in w_loads(k):
                c.wait()
            arrived(k % 4)
            x = feat[half_of(k), :, cut(k % 4)]
            for i, acc in enumerate((acc0, acc1)):
                add_dot(acc, x, wbuf[k % 3, i])

            @pl.when(k + 3 < 8)
            def _():
                for c in w_loads(k + 3):
                    c.start()

    def cot_step(lo, hi, arrived):
        @pl.loop(lo, hi)
        def _(k):
            wo_load(k).wait()
            arrived(k % 4)
            h = half_of(k)
            add_dot(acc2, cot[h, :, cut(k % 4)], wobuf[k % 3])
            flip(cot, cot_t, h, k % 4)

            @pl.when(k + 3 < 8)
            def _():
                wo_load(k + 3).start()

    @pl.loop(0, 4)
    def _(k):
        own(feat_hbm, feat, f_sem, k).wait()
        flip(feat, feat_t, tp, k)

    pl.semaphore_wait(barrier, 12)
    for k in range(4):
        give(feat_hbm, feat, f_ssem, f_rsem, k).start()
    for e in early:
        e.far()
    for k in range(4):
        give(cot_hbm, cot, c_ssem, c_rsem, k).start()
    for q in range(2):
        for e in early[1:]:
            e.near(q)
    project(0, 4, lambda k: None)
    cot_step(0, 4, lambda k: own(cot_hbm, cot, c_sem, k).wait())
    project(4, 8, lambda k: give(feat_hbm, feat, f_ssem, f_rsem, k).wait_recv())

    def gate_rows(at):
        kept = []
        for c in range(4):
            value = acc0[c, pl.ds(at, 32)].astype(BF16)
            gate = acc1[c, pl.ds(at, 32)].astype(BF16)
            vhalf[c, pl.ds(at, 32)] = value
            ghalf[c, pl.ds(at, 32)] = gate
            sig = jax.nn.sigmoid(gate.astype(F32))
            mixed = (value.astype(F32) * sig).astype(BF16)
            ext[c, pl.ds(at + 16, 32)] = mixed.astype(F32)
            kept.append(mixed)
        return kept

    def edge(send, recv, i, at):
        return remote(send.at[i], recv.at[i], e_ssem.at[at + i], e_rsem.at[at + i],
                      along(2 * i - 1))

    for i, kept in enumerate((gate_rows(0), gate_rows(480))):
        for c in range(4):
            edges[i, c] = kept[c][16 * i : 16 * i + 16]
    for i in range(2):
        edge(edges, edges_in, i, 0).start()
    for q in range(2):
        early[0].near(q)

    @pl.loop(1, 15)
    def _(b):
        gate_rows(pl.multiple_of(b * 32, 32))

    cot_step(4, 8, lambda k: give(cot_hbm, cot, c_ssem, c_rsem, k).wait_recv())

    def fill(buf, got, i):
        inside = sp > 0 if i == 0 else sp < 63
        for c in range(4):
            rows = got[1 - i, c].astype(F32)
            buf[c, 528 * i : 528 * i + 16] = jnp.where(inside, rows, 0.0)

    def conv(buf, c, at, first, step):
        total = jnp.zeros((64, 128), F32)
        for k in range(31):
            rows = buf[c, pl.ds(at + (first + step * k), 64)]
            total = total + taps[c, k : k + 1] * rows
        return total

    def share(n):
        return remote(stats.at[n], stats_in.at[n], s_ssem.at[n], s_rsem.at[n], partner())

    def conv_rows(b):
        at = pl.multiple_of(b * 64, 64)
        zero = jnp.zeros((64, 128), F32)

        @pl.loop(0, 4, init_carry=(zero, zero))
        def totals(c, carry):
            got = conv(ext, c, at, 1, 1)
            acc0[c, pl.ds(at, 64)] = got
            return carry[0] + got, carry[1] + got * got

        stats[0, 0, pl.ds(at, 64)] = totals[0]
        stats[0, 1, pl.ds(at, 64)] = totals[1]

    pl.loop(1, 7)(conv_rows)
    for i in range(2):
        edge(edges, edges_in, 1 - i, 0).wait_recv()
        fill(ext, edges_in, i)

    pl.loop(0, 8, step=7)(conv_rows)
    share(0).start()

    @pl.loop(0, 4)
    def _(k):
        flip(feat, feat_t, 1 - tp, k)

    share(0).wait_recv()

    none = jnp.zeros((8, 128), F32)

    @pl.loop(0, 16, init_carry=(none,) * 4)
    def gain_sums(b, carry):
        at = pl.multiple_of(b * 32, 32)
        rows = pl.ds(at, 32)
        mean = lane_sum(stats[0, 0, rows] + stats_in[0, 0, rows]) / 1024
        square = lane_sum(stats[0, 1, rows] + stats_in[0, 1, rows]) / 1024
        inv = lax.rsqrt(square - mean * mean + NORM_EPS)
        inv_rows[rows] = jnp.broadcast_to(inv, (32, 128))
        first = jnp.zeros((32, 128), F32)
        second = jnp.zeros((32, 128), F32)
        carried = []
        for c in range(4):
            gain = gains[c, 0:1]
            normed = (acc0[c, rows] - mean) * inv
            pre = normed * gain
            sig = jax.nn.sigmoid(pre)
            act[rows, 128 * c : 128 * c + 128] = (pre * sig).astype(BF16)
            grad = acc2[c, rows] * sig * (1.0 + pre * (1.0 - sig))
            carried.append(carry[c] + fold(grad * normed))
            ngrad = grad * gain
            acc0[c, rows] = normed
            acc1[c, rows] = ngrad
            first = first + ngrad
            second = second + ngrad * normed
        stats[1, 0, rows] = first
        stats[1, 1, rows] = second
        return tuple(carried)

    share(1).start()
    for c in range(4):
        cols[c, 31:32] = jnp.sum(gain_sums[c], axis=0, keepdims=True)
    run("first", out_parts[1:2], 0)
    share(1).wait_recv()

    def conv_grad(at):
        rows = pl.ds(at, 32)
        m1 = lane_sum(stats[1, 0, rows] + stats_in[1, 0, rows]) / 1024
        m2 = lane_sum(stats[1, 1, rows] + stats_in[1, 1, rows]) / 1024
        kept = []
        for c in range(4):
            got = inv_rows[rows] * (acc1[c, rows] - m1 - acc0[c, rows] * m2)
            gext[c, pl.ds(at + 16, 32)] = got
            kept.append(got)
        return kept

    for i, kept in enumerate((conv_grad(0), conv_grad(480))):
        for c in range(4):
            gedges[i, c] = kept[c][16 * i : 16 * i + 16]
    for i in range(2):
        edge(gedges, gedges_in, i, 2).start()

    start_round((out_parts[0], out_parts[2]))

    @pl.loop(1, 15)
    def _(b):
        conv_grad(pl.multiple_of(b * 32, 32))

    def grad_rows(b):
        at = pl.multiple_of(b * 64, 64)
        rows = pl.ds(at, 64)

        @pl.loop(0, 4)
        def _(c):
            mixed_grad = conv(gext, c, at, 31, -1)
            value = vhalf[c, rows].astype(F32)
            sig = jax.nn.sigmoid(ghalf[c, rows].astype(F32))
            vgrad = mixed_grad * sig
            ggrad = mixed_grad * value * sig * (1.0 - sig)
            acc0[c, rows] = vgrad
            acc1[c, rows] = ggrad
            lanes = pl.ds(pl.multiple_of(c * 128, 128), 128)
            vlow[rows, lanes] = vgrad.astype(BF16)
            glow[rows, lanes] = ggrad.astype(BF16)

    for e in early:
        for slot in range(2):
            e.share(slot)
    pl.loop(1, 7)(grad_rows)
    for i in range(2):
        edge(gedges, gedges_in, 1 - i, 2).wait_recv()
        fill(gext, gedges_in, i)

    pl.loop(0, 8, step=7)(grad_rows)

    def store(i, c):
        src, dst = ((acc0, vgrad_hbm), (acc1, ggrad_hbm))[i]
        return pltpu.make_async_copy(
            src.at[c], dst.at[:, 128 * c : 128 * c + 128], o_sem.at[i, c]
        )

    def leave(i):
        src = (value_out, gate_out, out_out, small_out)[i]
        dst = (vw_hbm, gw_hbm, ow_hbm, small_hbm)[i]
        return pltpu.make_async_copy(src, dst, r_sem.at[i])

    for i in range(2):
        for c in range(4):
            store(i, c).start()

    run("first", value_parts, 0)
    run("first", gate_parts, 0)
    early[0].pass_on()
    early[2].pass_on()
    early[1].pass_on()
    run("second", [out_parts[p] for p in (0, 2)], 0)
    @pl.loop(0, 4)
    def _(c):
        @pl.loop(0, 16, init_carry=(none,) * 31)
        def tap_sums(b, carry):
            at = pl.multiple_of(b * 32, 32)
            grad = gext[c, pl.ds(at + 16, 32)]
            return tuple(
                carry[k] + fold(grad * ext[c, pl.ds(at + (k + 1), 32)]) for k in range(31)
            )

        for k in range(31):
            cols[c, k : k + 1] = jnp.sum(tap_sums[k], axis=0, keepdims=True)

    tiny.send(0)

    out_parts[1].second(0)
    value_parts[0].second(0)
    early[0].have(0)
    early[0].have(1)
    value_parts[0].middle(0)
    value_parts[2].second(0)
    early[2].have(0)
    early[2].have(1)
    value_parts[2].middle(0)
    value_parts[1].second(0)
    early[1].have(0)
    early[1].have(1)
    value_parts[1].middle(0)
    gate_parts[0].second(0)
    gate_parts[0].middle(0)
    run("second", [gate_parts[p] for p in (2, 1)], 0)
    run("middle", [gate_parts[p] for p in (2, 1)], 0)
    early[0].share(2)
    out_parts[0].third(0)
    tiny.collect(0)
    tiny.send(1)
    early[1].share(2)
    out_parts[0].first(1)
    out_parts[2].third(0)
    out_parts[2].first(1)
    early[0].have(2)
    value_parts[0].third(0)
    early[2].share(2)
    value_parts[0].first(1)
    out_parts[1].third(0)
    out_parts[1].first(1)
    gate_parts[0].third(0)
    early[2].have(2)
    value_parts[2].third(0)
    value_parts[2].first(1)
    early[1].have(2)
    value_parts[1].third(0)
    gate_parts[0].first(1)
    value_parts[1].first(1)
    gate_parts[1].third(0)
    gate_parts[1].first(1)
    gate_parts[2].third(0)
    value_parts[0].second(1)
    out_parts[0].second(1)
    gate_parts[2].first(1)
    run("second", [out_parts[p] for p in (2, 1)], 1)
    tiny.collect(1)
    tiny.send(2)
    run("second", [value_parts[p] for p in (2, 1)], 1)
    run("second", gate_parts, 1)
    value_parts[0].third(1)
    out_parts[0].third(1)
    value_parts[0].first(2)
    out_parts[0].first(2)
    out_parts[2].third(1)
    out_parts[2].first(2)
    out_parts[1].third(1)
    out_parts[1].first(2)
    value_parts[1].third(1)
    value_parts[1].first(2)
    value_parts[2].third(1)
    value_parts[2].first(2)
    gate_parts[0].third(1)
    gate_parts[0].first(2)
    gate_parts[1].third(1)
    gate_parts[1].first(2)
    gate_parts[2].third(1)
    gate_parts[2].first(2)
    value_parts[0].third(2)
    tiny.collect(2)
    tiny.send(3)
    out_parts[2].third(2)
    out_parts[0].third(2)
    out_parts[1].third(2)
    leave(2).start()
    value_parts[1].third(2)
    value_parts[2].third(2)
    leave(0).start()
    gate_parts[0].third(2)
    gate_parts[1].third(2)
    gate_parts[2].third(2)
    leave(1).start()
    tiny.collect(3)
    leave(3).start()

    tiny.drain()
    for e in early:
        e.drain()
    for part in (*out_parts, *value_parts, *gate_parts):
        for stage in range(3):
            part.drain(stage)
    for k in range(4):
        give(feat_hbm, feat, f_ssem, f_rsem, k).wait_send()
        give(cot_hbm, cot, c_ssem, c_rsem, k).wait_send()
    for i in range(2):
        edge(edges, edges_in, i, 0).wait_send()
        edge(gedges, gedges_in, i, 2).wait_send()
        share(i).wait_send()
        for c in range(4):
            store(i, c).wait()
    for i in range(4):
        leave(i).wait()


def hand_kernel(vgrad, ggrad, vw, gw, ow, small, vgrad_o, ggrad_o, vw_o, gw_o, ow_o,
                taps_o, gain_o, big, mid, tiny, taps, gain, in_sem, out_sem):
    moves = []
    for i, (src, dst) in enumerate(((vgrad, vgrad_o), (ggrad, ggrad_o))):
        for q in range(4):
            rows = pl.ds(q * 128, 128)
            moves.append((src.at[rows], big.at[i, rows], [(big.at[i, rows], dst.at[rows])]))
    for i, (src, dst) in enumerate(((vw, vw_o), (gw, gw_o), (ow, ow_o))):
        moves.append((src, mid.at[i], [(mid.at[i], dst)]))
    moves.append((small, tiny, [(taps, taps_o), (gain, gain_o)]))
    ins = [
        pltpu.make_async_copy(src, held, in_sem.at[i]) for i, (src, held, _) in enumerate(moves)
    ]
    outs, at = [], 0
    for copy in ins:
        copy.start()
    for copy, (_, _, goes) in zip(ins, moves):
        copy.wait()
        if len(goes) == 2:
            taps[...] = tiny[0:31]
            gain[...] = tiny[31:32]
        for src, dst in goes:
            outs.append(pltpu.make_async_copy(src, dst, out_sem.at[at]))
            outs[-1].start()
            at += 1
    for copy in outs:
        copy.wait()


def on_device(features, weight_value, weight_gate, weight_out, conv_taps, norm_gain, out_grad):
    grad = jax.ShapeDtypeStruct((512, 512), F32)
    piece = jax.ShapeDtypeStruct((64, 512), F32)
    vmem = pl.BlockSpec(memory_space=pltpu.VMEM)
    hbm = pl.BlockSpec(memory_space=pl.ANY)
    dma = pltpu.SemaphoreType.DMA
    tiles = (4, 512, 128)
    vgrad, ggrad, vw, gw, ow, small = pl.pallas_call(
        whole_kernel,
        out_shape=(grad, grad, piece, piece, piece, jax.ShapeDtypeStruct((32, 512), F32)),
        in_specs=[hbm, hbm, hbm, hbm, vmem, vmem, hbm],
        out_specs=(hbm,) * 6,
        scratch_shapes=[
            *[pltpu.VMEM((64, 512), F32)] * 3,
            pltpu.VMEM((32, 512), F32),
            pltpu.VMEM((2, 512, 2048), BF16),
            pltpu.VMEM((2, 512, 2048), BF16),
            pltpu.VMEM((4, 4, 4, 64, 512), BF16),
            pltpu.VMEM((4, 4, 4, 64, 512), BF16),
            pltpu.VMEM((3, 2, 512, 512), BF16),
            pltpu.VMEM((3, 512, 512), BF16),
            pltpu.VMEM(tiles, F32),
            pltpu.VMEM(tiles, F32),
            pltpu.VMEM(tiles, F32),
            pltpu.VMEM(tiles, BF16),
            pltpu.VMEM(tiles, BF16),
            pltpu.VMEM((4, 544, 128), F32),
            pltpu.VMEM((4, 544, 128), F32),
            pltpu.VMEM((4, 32, 128), F32),
            pltpu.VMEM((4, 8, 128), F32),
            pltpu.VMEM((512, 512), BF16),
            pltpu.VMEM((512, 512), BF16),
            pltpu.VMEM((512, 512), BF16),
            pltpu.VMEM((2, 4, 16, 128), BF16),
            pltpu.VMEM((2, 4, 16, 128), BF16),
            pltpu.VMEM((2, 4, 16, 128), F32),
            pltpu.VMEM((2, 4, 16, 128), F32),
            pltpu.VMEM((2, 2, 512, 128), F32),
            pltpu.VMEM((2, 2, 512, 128), F32),
            pltpu.VMEM((512, 128), F32),
            pltpu.VMEM((4, 32, 128), F32),
            pltpu.VMEM((4, 4, 32, 128), F32),
            pltpu.VMEM((3, 32, 128), F32),
            dma((3, 2)), dma((3,)),
            dma((4,)), dma((4,)), dma((4,)),
            dma((4,)), dma((4,)), dma((4,)),
            dma((4,)), dma((4,)), dma((2,)), dma((2,)), dma((2, 4)), dma((4,)),
            dma((16,)), dma((16,)),
            *early_scratch(),
            *part_scratch(),
        ],
        compiler_params=pltpu.CompilerParams(
            collective_id=0, has_side_effects=True, vmem_limit_bytes=64 * 1024 * 1024 - 65536
        ),
    )(features, weight_value, weight_gate, weight_out, conv_taps, norm_gain[None], out_grad)
    *rest, gain = pl.pallas_call(
        hand_kernel,
        out_shape=(
            grad, grad, piece, piece, piece,
            jax.ShapeDtypeStruct((31, 512), F32), jax.ShapeDtypeStruct((1, 512), F32),
        ),
        in_specs=[hbm] * 6,
        out_specs=(hbm,) * 7,
        scratch_shapes=[
            pltpu.VMEM((2, 512, 512), F32),
            pltpu.VMEM((3, 64, 512), F32),
            pltpu.VMEM((32, 512), F32),
            pltpu.VMEM((31, 512), F32),
            pltpu.VMEM((1, 512), F32),
            dma((12,)), dma((13,)),
        ],
    )(vgrad, ggrad, vw, gw, ow, small)
    return (*rest, gain[0])


def solution(mesh):
    return jax.shard_map(
        on_device,
        mesh=mesh,
        in_specs=(
            P(SP, "tp"), P(None, "tp"), P(None, "tp"), P(None, "tp"),
            P(None, "tp"), P("tp"), P(SP, "tp"),
        ),
        out_specs=(
            P(SP, "tp"), P(SP, "tp"), P(SP, "tp"), P(SP, "tp"), P(SP, "tp"),
            P(None, "tp"), P("tp"),
        ),
        check_vma=False,
    )
```
